128 devices in a mesh: sp: 64 (over z, y, x), tp: 2 (over core).
Axes of the slice: x: 4, y: 4, z: 4, core: 2. Of those that a mesh axis runs over, the one named last changes fastest.
Arguments:
- stream: bfloat16 [32768, 2048], P(('sp', 'tp')), may hold values from -6 to 6
- queries: bfloat16 [32768, 512], P('sp', 'tp'), may hold values from -6 to 6
- key_rows: bfloat16 [32768, 512], P('sp', 'tp'), may hold values from -6 to 6
- value_rows: bfloat16 [32768, 1024], P('sp', 'tp'), may hold values from -6 to 6
- out_gate: bfloat16 [32768, 1024], P('sp', 'tp'), may hold values from -6 to 6
- in_gate: float32 [4, 32768], P('tp', 'sp'), may hold values from -4 to 214
- forget_gate: float32 [4, 32768], P('tp', 'sp'), may hold values from -2 to 20
- out_proj: bfloat16 [1024, 2048], replicated, may hold values from -0.1875 to 0.1875
- ffn_gain: float32 [2048], replicated, may hold values from 0.1 to 1.9
- gate_proj: bfloat16 [64, 2048, 768], P('sp', None, 'tp'), may hold values from -0.125 to 0.125
- up_proj: bfloat16 [64, 2048, 768], P('sp', None, 'tp'), may hold values from -0.125 to 0.125
- down_proj: bfloat16 [64, 768, 2048], P('sp', 'tp'), may hold values from -0.21875 to 0.21875
- expert_ids: int32 [32768, 2], P(('sp', 'tp')), may hold values from 0 to 63, as said below
- route_weights: float32 [32768, 2], P(('sp', 'tp')), may hold values from 0.05 to 1
Outputs:
- result_stream: bfloat16 [32768, 2048], P(('sp', 'tp'))
The draws below stay inside these ranges and needn't reach their ends.
Inputs may be any that keep to these rules, and one draw needn't show every extreme that they name: `expert_ids`: both experts of a row are different and lie in one group (expert // 8 equal). In the rows of one device (aligned blocks of 256 rows) each expert is named at most 16 times, some expert exactly 16 times, and each expert shares its rows with a single partner.
All inputs are finite; a program needn't handle non-finite values.
Results may differ from the reference program's by a relative error of at most 0.012.
Values may be sent and summed in bfloat16 or wider, within the bound.
A program may use at most 128 MiB of HBM per device.

```python
import jax
import jax.numpy as jnp
from jax import lax

D = 2048
HEADS = 4
QK = 128
V_DIM = 256
FF = 768
GROUP = 8
TOPK = 2
BLOCK = 64
TOK_DEV = 512
TOKENS = 32768
EXPERTS = 64
ROWS = 256
CAP = 16
N_SP = 64
N_TP = 2


def draw_in_gate(key, part):
    base = jnp.clip(jax.random.normal(jax.random.fold_in(key, 3), (HEADS, TOKENS), jnp.float32), -4.0, 4.0)
    return base


def draw_forget_gate(key, part):
    order_key = jax.random.fold_in(key, 5)
    device_key = jax.random.fold_in(key, 6)
    block_key = jax.random.fold_in(key, 7)
    noise_key = jax.random.fold_in(key, 8)
    order = jax.random.permutation(order_key, HEADS)
    quick = order < HEADS // 2
    base = jnp.where(quick, 1.0 / 40.0, 0.5 / TOKENS).astype(jnp.float32)
    device_factor = jnp.exp(jax.random.uniform(device_key, (HEADS, TOKENS // TOK_DEV), jnp.float32, jnp.log(0.4), jnp.log(2.5)))
    block_factor = jnp.exp(jax.random.uniform(block_key, (HEADS, TOKENS // BLOCK), jnp.float32, jnp.log(0.7), jnp.log(1.4)))
    noise = jnp.clip(jax.random.normal(noise_key, (HEADS, TOKENS), jnp.float32), -3.0, 3.0)
    rate = base[:, None] * jnp.repeat(device_factor, TOK_DEV, axis=1) * jnp.repeat(block_factor, BLOCK, axis=1) * jnp.exp(0.5 * noise)
    return -jnp.log(rate)


def route_table(key):
    groups = EXPERTS // GROUP
    pairs = EXPERTS // 2
    slot_total = pairs * CAP
    star_key = jax.random.fold_in(key, 21)
    share_key = jax.random.fold_in(key, 22)
    blocks_key = jax.random.fold_in(key, 23)
    star = jax.random.randint(star_key, (), 0, EXPERTS)
    shared = jax.random.randint(share_key, (EXPERTS,), 0, 3)

    def one_block(block_key):
        pair_key, prio_key, tie_key, shuffle_key, flip_key = jax.random.split(block_key, 5)
        group_keys = jax.random.split(pair_key, groups)
        perms = jax.vmap(lambda group_key: jax.random.permutation(group_key, GROUP))(group_keys)
        members = perms + (jnp.arange(groups, dtype=jnp.int32) * GROUP)[:, None]
        first = members[:, 0::2].reshape(-1)
        second = members[:, 1::2].reshape(-1)
        priority = jnp.maximum(shared[first], shared[second]) + jax.random.randint(prio_key, (pairs,), 0, 3)
        priority = jnp.where((first == star) | (second == star), 100, priority)
        tie = jax.random.permutation(tie_key, slot_total)
        score = priority[jnp.arange(slot_total) // CAP] * slot_total + tie
        _, chosen = lax.top_k(score, ROWS)
        chosen = jax.random.permutation(shuffle_key, chosen)
        pair = chosen // CAP
        flip = jax.random.randint(flip_key, (ROWS,), 0, 2)
        left = first[pair]
        right = second[pair]
        return jnp.stack([jnp.where(flip == 1, right, left), jnp.where(flip == 1, left, right)], axis=1)
    table = jax.vmap(one_block)(jax.random.split(blocks_key, TOKENS // ROWS))
    return table.reshape(TOKENS, 2).astype(jnp.int32)


def draw_expert_ids(key, part):
    return route_table(jax.random.fold_in(key, 11))


def level_of(stream_key, dims, shards, low, high):
    def one(dim, parts):
        heights = jax.random.uniform(jax.random.fold_in(jax.random.fold_in(stream_key, 6), dim), (parts,), jnp.float32, low / len(shards), high / len(shards))
        return jnp.repeat(jnp.exp(heights), dims[dim] // parts).reshape((-1,) + (1,) * (len(dims) - dim - 1))

    gain = one(*shards[0])
    for cut in shards[1:]:
        gain = gain * one(*cut)
    return gain


def bell_draw(rng, shape, scale, most, shards=(), kind=jnp.bfloat16):
    values = scale * jax.random.normal(rng, shape, jnp.float32)
    if shards:
        values = values * level_of(rng, shape, shards, -0.22, 0.18)
    return jnp.clip(values, -most, most).astype(kind)


def setup_inputs(seed: int = 0) -> dict:
    keys = jax.random.split(jax.random.key(seed), 15)
    return {
        "stream": bell_draw(keys[0], (TOKENS, D), 1.0, 6.0, ((0, 128),)),
        "queries": bell_draw(keys[1], (TOKENS, HEADS * QK), 1.0, 6.0, ((0, 64), (1, 2))),
        "key_rows": bell_draw(keys[2], (TOKENS, HEADS * QK), 1.0, 6.0, ((0, 64), (1, 2))),
        "value_rows": bell_draw(keys[3], (TOKENS, HEADS * V_DIM), 1.0, 6.0, ((0, 64), (1, 2))),
        "out_gate": bell_draw(keys[4], (TOKENS, HEADS * V_DIM), 1.0, 6.0, ((0, 64), (1, 2))),
        "in_gate": draw_in_gate(jax.random.fold_in(keys[14], 71), 0),
        "forget_gate": draw_forget_gate(jax.random.fold_in(keys[14], 71), 0),
        "out_proj": bell_draw(keys[7], (HEADS * V_DIM, D), (HEADS * V_DIM) ** -0.5, 0.1875),
        "ffn_gain": jnp.clip(1.0 + 0.18 * jax.random.normal(keys[8], (D,), jnp.float32), 0.1, 1.9),
        "gate_proj": bell_draw(keys[9], (EXPERTS, D, FF), D ** -0.5, 0.125, ((0, 64), (2, 2))),
        "up_proj": bell_draw(keys[10], (EXPERTS, D, FF), D ** -0.5, 0.125, ((0, 64), (2, 2))),
        "down_proj": bell_draw(keys[11], (EXPERTS, FF, D), FF ** -0.5, 0.21875, ((0, 64), (1, 2))),
        "expert_ids": draw_expert_ids(jax.random.fold_in(keys[14], 71), 0),
        "route_weights": jnp.clip(0.05 + 0.95 * jax.random.uniform(keys[13], (TOKENS, TOPK), jnp.float32) ** level_of(keys[13], (TOKENS, TOPK), ((0, 128),), -0.2, 0.2), 0.05, 1.0),
    }


epsilon = 1e-06

def mechanism(queries, key_rows, value_rows, in_gate, forget_gate):
    heads, length = in_gate.shape
    blocks = length // BLOCK

    def per_head(rows, size):
        return rows.astype(jnp.float32).reshape(blocks, BLOCK, heads, size).transpose(2, 0, 1, 3)
    query_blocks = per_head(queries, QK)
    key_blocks = per_head(key_rows, QK) * QK ** (-0.5)
    value_blocks = per_head(value_rows, V_DIM)
    input_gate = in_gate.reshape(heads, blocks, BLOCK)
    cumulative = jnp.cumsum(jax.nn.log_sigmoid(forget_gate).reshape(heads, blocks, BLOCK), axis=-1)
    closing = cumulative[..., -1]
    causal = jnp.tril(jnp.ones((BLOCK, BLOCK), dtype=bool))
    log_inner = jnp.where(causal, cumulative[..., :, None] - cumulative[..., None, :] + input_gate[..., None, :], -jnp.inf)
    log_close = closing[..., None] - cumulative + input_gate

    def advance(carry, inputs):
        state, level = carry
        key_block, value_block, close_block, last_block = inputs
        new_level = jnp.maximum(last_block + level, lax.optimization_barrier(jnp.max(close_block, axis=-1)))
        weight = jnp.exp(close_block - new_level[:, None])
        update = jnp.einsum('hl,hld,hle->hde', weight, key_block, value_block, precision=lax.Precision.HIGHEST)
        new_state = state * jnp.exp(last_block + level - new_level)[:, None, None] + update
        return ((new_state, new_level), (state, level))
    start = (jnp.zeros((heads, QK, V_DIM), jnp.float32), jnp.zeros((heads,), jnp.float32))
    _, (states, levels) = lax.scan(advance, start, (jnp.moveaxis(key_blocks, 1, 0), jnp.moveaxis(value_blocks, 1, 0), jnp.moveaxis(log_close, 1, 0), closing.T))
    states = jnp.moveaxis(states, 0, 1)
    levels = levels.T
    log_inter = cumulative + levels[..., None]
    peak = jnp.maximum(log_inter, lax.optimization_barrier(jnp.max(log_inner, axis=-1)))
    scores = jnp.einsum('hntd,hnsd->hnts', query_blocks, key_blocks, precision=lax.Precision.HIGHEST) * jnp.exp(log_inner - peak[..., None])
    carried = jnp.einsum('hntd,hnde->hnte', query_blocks, states, precision=lax.Precision.HIGHEST)
    local = jnp.einsum('hnts,hnse->hnte', scores, value_blocks, precision=lax.Precision.HIGHEST)
    numerator = jnp.exp(log_inter - peak)[..., None] * carried + local
    return numerator.transpose(1, 2, 0, 3).reshape(length, heads, V_DIM)

def reference(stream, queries, key_rows, value_rows, out_gate, in_gate, forget_gate, out_proj, ffn_gain, gate_proj, up_proj, down_proj, expert_ids, route_weights):
    numerator = mechanism(queries, key_rows, value_rows, in_gate, forget_gate)
    length, heads, _ = numerator.shape
    scaled = numerator * lax.rsqrt(lax.optimization_barrier(jnp.mean(numerator * numerator, axis=-1, keepdims=True)) + epsilon)
    gated = scaled.reshape(length, heads * V_DIM) * jax.nn.sigmoid(out_gate.astype(jnp.float32))
    heads_out = gated.astype(jnp.bfloat16)
    mix = jnp.dot(heads_out, out_proj, preferred_element_type=jnp.float32)
    middle = (stream.astype(jnp.float32) + mix).astype(jnp.bfloat16)
    middle_float = middle.astype(jnp.float32)
    normed = (middle_float * lax.rsqrt(lax.optimization_barrier(jnp.mean(middle_float * middle_float, axis=-1, keepdims=True)) + epsilon) * ffn_gain.astype(jnp.float32)).astype(jnp.bfloat16)
    flat_ids = expert_ids.reshape(-1).astype(jnp.int32)
    flat_weights = route_weights.reshape(-1).astype(jnp.float32)
    flat_tokens = (jnp.arange(TOKENS * TOPK, dtype=jnp.int32) // TOPK).astype(jnp.int32)
    most = N_SP * N_TP * CAP

    def expert_step(total, inputs):
        gate_weight, up_weight, down_weight, index = inputs
        chosen = jnp.nonzero(flat_ids == index, size=most, fill_value=0)[0].astype(jnp.int32)
        amount = jnp.sum((flat_ids == index).astype(jnp.int32))
        live = (jnp.arange(most, dtype=jnp.int32) < amount).astype(jnp.float32)
        owners = flat_tokens[chosen]
        rows = normed[owners]
        hidden = (jax.nn.silu(jnp.dot(rows, gate_weight, preferred_element_type=jnp.float32)) * jnp.dot(rows, up_weight, preferred_element_type=jnp.float32)).astype(jnp.bfloat16)
        output = jnp.dot(hidden, down_weight, preferred_element_type=jnp.float32).astype(jnp.bfloat16).astype(jnp.float32)
        contribution = output * (flat_weights[chosen] * live)[:, None]
        return (total.at[owners].add(contribution), None)
    total, _ = lax.scan(expert_step, jnp.zeros((TOKENS, D), jnp.float32), (gate_proj, up_proj, down_proj, jnp.arange(EXPERTS, dtype=jnp.int32)))
    return (middle_float + total).astype(jnp.bfloat16)
```

```python
import jax
import jax.numpy as jnp
from jax import lax
from jax.experimental import pallas as pl
from jax.experimental.pallas import tpu as pltpu
from jax.sharding import Mesh
from jax.sharding import PartitionSpec as P

MESH = pl.DeviceIdType.MESH
QK = 128
V_DIM = 256
BLOCK = 64
SP = ("sp_0", "sp_1", "sp_2")
SP_TP = ("sp_0", "sp_1", "sp_2", "tp")


epsilon = 1e-06
floor_level = -1e30


def neutral_like(array, identity):
    return jax.tree.map(
        lambda a, e: jnp.broadcast_to(jnp.asarray(e, a.dtype), a.shape), array, identity
    )


def gathered_once(array, axis):
    leaves = jax.tree.leaves(array)
    sequence = sorted(range(len(leaves)), key=lambda k: -leaves[k].size)
    width = (1, *leaves[sequence[0]].shape)[-1]
    lines = [
        jnp.pad(leaves[k].reshape(-1), (0, -leaves[k].size % width)).reshape(-1, width)
        for k in sequence
    ]
    both, at, found = (lax.all_gather(jnp.concatenate(lines), axis), 0, {})
    for k, line in zip(sequence, lines):
        share = both[:, at : at + len(line)].reshape(len(both), -1)
        found[k] = share[:, : leaves[k].size].reshape(-1, *leaves[k].shape)
        at += len(line)
    numbers = iter(range(len(leaves)))
    return jax.tree.map(lambda _: found[next(numbers)], array)


def prefix_by_axis(array, axes, combine, identity):
    before = start = neutral_like(array, identity)
    total = array
    for axis in reversed(axes):
        count, position = (lax.axis_size(axis), lax.axis_index(axis))
        pieces = gathered_once(total, axis)
        inside, total = (start, start)
        for k in range(count):
            passed = k < position
            total = combine(total, jax.tree.map(lambda part: part[k], pieces))
            inside = jax.tree.map(lambda new, old: jnp.where(passed, new, old), total, inside)
        before = combine(inside, before)
    return before


def join_states(earlier, later):
    early_state, early_level, early_decay = earlier
    late_state, late_level, late_decay = later
    level = jnp.maximum(late_decay + early_level, late_level)
    state = (
        early_state * jnp.exp(late_decay + early_level - level)[:, None, None]
        + late_state * jnp.exp(late_level - level)[:, None, None]
    )
    return (state, level, early_decay + late_decay)


OFFSETS = sorted(
    ((a, b, c) for a in range(4) for b in range(4) for c in range(4)),
    key=lambda o: sum(min(v, 4 - v) for v in o),
)
SLOT = 16
GROUP_ROWS = 256
PER_GROUP = GROUP_ROWS // SLOT


def place():
    return [lax.axis_index(axis) for axis in SP_TP]


def peer(here, offset, sign=1):
    z, y, x, core = here
    return tuple(lax.rem(p + (sign * o) % 4, 4) for p, o in zip((z, y, x), offset)) + (core,)


def experts_kernel(
    select_ref,
    weigh_ref,
    normed_ref,
    middle_ref,
    gate_ref,
    up_ref,
    down_ref,
    out_ref,
    outgoing,
    arrived,
    answers,
    returned,
    gate_full,
    up_full,
    down_full,
    hidden,
    total,
    local_sem,
    weight_send,
    weight_recv,
    send_sem,
    recv_sem,
    back_send,
    back_recv,
):
    here = place()
    other = (here[0], here[1], here[2], 1 - here[3])
    barrier = pltpu.get_barrier_semaphore()
    for offset in OFFSETS[1:]:
        pl.semaphore_signal(barrier, inc=1, device_id=peer(here, offset), device_id_type=MESH)
    pl.semaphore_signal(barrier, inc=1, device_id=other, device_id_type=MESH)
    half = gate_ref.shape[1]
    locals_ = [
        pltpu.make_async_copy(gate_ref, gate_full.at[:, pl.ds(0, half)], local_sem.at[0]),
        pltpu.make_async_copy(up_ref, up_full.at[:, pl.ds(0, half)], local_sem.at[1]),
        pltpu.make_async_copy(down_ref, down_full.at[pl.ds(0, half)], local_sem.at[2]),
    ]
    for copy in locals_:
        copy.start()

    def rows(i):
        return pl.ds(i * SLOT, SLOT)

    def group(g):
        return pl.ds(g * GROUP_ROWS, GROUP_ROWS)

    groups = len(OFFSETS) // PER_GROUP
    tile = 256

    def build(g):
        pick = select_ref[group(g), :]
        for n in range(0, outgoing.shape[1], tile):
            cols = slice(n, n + tile)
            outgoing[group(g), cols] = jnp.dot(
                pick, normed_ref[:, cols], preferred_element_type=jnp.float32
            ).astype(jnp.bfloat16)

    def send(g):
        for i in range(max(g * PER_GROUP, 1), (g + 1) * PER_GROUP):
            pltpu.make_async_remote_copy(
                src_ref=outgoing.at[rows(i)],
                dst_ref=arrived.at[rows(i)],
                send_sem=send_sem,
                recv_sem=recv_sem.at[g],
                device_id=peer(here, OFFSETS[i]),
                device_id_type=MESH,
            ).start()

    build(0)
    pl.semaphore_wait(barrier, len(OFFSETS))
    weights = [
        pltpu.make_async_remote_copy(
            src_ref=mine,
            dst_ref=theirs,
            send_sem=weight_send.at[i],
            recv_sem=weight_recv.at[i],
            device_id=other,
            device_id_type=MESH,
        )
        for i, (mine, theirs) in enumerate(
            (
                (gate_ref, gate_full.at[:, pl.ds(half, half)]),
                (up_ref, up_full.at[:, pl.ds(half, half)]),
                (down_ref, down_full.at[pl.ds(half, half)]),
            )
        )
    ]
    for g in range(1, groups):
        build(g)
        send(g - 1)
        if g == 1:
            for copy in weights:
                copy.start()
    arrived[rows(0), :] = outgoing[rows(0), :]
    send(groups - 1)

    def landed(ref, sem, first, last):
        span = pl.ds(first * SLOT, (last - first) * SLOT)
        pltpu.make_async_copy(ref.at[span], ref.at[span], sem).wait()

    for copy in locals_:
        copy.wait()
    for copy in weights:
        copy.wait_recv()
    for g in range(groups):
        landed(arrived, recv_sem.at[g], max(g * PER_GROUP, 1), (g + 1) * PER_GROUP)
        block = arrived[group(g), :]
        for n in range(0, hidden.shape[1], tile):
            cols = slice(n, n + tile)
            gates = jnp.dot(block, gate_full[:, cols], preferred_element_type=jnp.float32)
            ups = jnp.dot(block, up_full[:, cols], preferred_element_type=jnp.float32)
            hidden[:, cols] = (gates * jax.nn.sigmoid(gates) * ups).astype(jnp.bfloat16)
        for n in range(0, answers.shape[1], tile):
            cols = slice(n, n + tile)
            answers[group(g), cols] = jnp.dot(
                hidden[...], down_full[:, cols], preferred_element_type=jnp.float32
            ).astype(jnp.bfloat16)
        for i in range(max(g * PER_GROUP, 1), (g + 1) * PER_GROUP):
            pltpu.make_async_remote_copy(
                src_ref=answers.at[rows(i)],
                dst_ref=returned.at[rows(i)],
                send_sem=back_send,
                recv_sem=back_recv.at[g],
                device_id=peer(here, OFFSETS[i], -1),
                device_id_type=MESH,
            ).start()
    returned[rows(0), :] = answers[rows(0), :]
    for g in range(groups):
        landed(returned, back_recv.at[g], max(g * PER_GROUP, 1), (g + 1) * PER_GROUP)
        for n in range(0, out_ref.shape[1], tile):
            cols = slice(n, n + tile)
            part = jnp.dot(
                weigh_ref[0, :, group(g)],
                returned[group(g), cols],
                preferred_element_type=jnp.float32,
            ) + jnp.dot(
                weigh_ref[1, :, group(g)],
                returned[group(g), cols],
                preferred_element_type=jnp.float32,
            )
            before = middle_ref[:, cols].astype(jnp.float32) if g == 0 else total[:, cols]
            if g < groups - 1:
                total[:, cols] = before + part
            else:
                out_ref[:, cols] = (before + part).astype(jnp.bfloat16)
    landed(outgoing, send_sem, 1, len(OFFSETS))
    landed(answers, back_send, 1, len(OFFSETS))
    for copy in weights:
        copy.wait_send()


def experts(select, weigh, normed, middle, gate, up, down):
    rows_here, width = normed.shape
    slots = select.shape[0]
    half = gate.shape[1]
    vmem = pl.BlockSpec(memory_space=pltpu.VMEM)
    hbm = pl.BlockSpec(memory_space=pl.ANY)
    dma = pltpu.SemaphoreType.DMA
    groups = slots // GROUP_ROWS
    return pl.pallas_call(
        experts_kernel,
        out_shape=jax.ShapeDtypeStruct((rows_here, width), jnp.bfloat16),
        in_specs=[vmem] * 4 + [hbm] * 3,
        out_specs=vmem,
        scratch_shapes=[pltpu.VMEM((slots, width), jnp.bfloat16)] * 4
        + [
            pltpu.VMEM((width, 2 * half), jnp.bfloat16),
            pltpu.VMEM((width, 2 * half), jnp.bfloat16),
            pltpu.VMEM((2 * half, width), jnp.bfloat16),
            pltpu.VMEM((GROUP_ROWS, 2 * half), jnp.bfloat16),
            pltpu.VMEM((rows_here, width), jnp.float32),
            dma((3,)),
            dma((3,)),
            dma((3,)),
            dma(()),
            dma((groups,)),
            dma(()),
            dma((groups,)),
        ],
        compiler_params=pltpu.CompilerParams(
            collective_id=1, has_side_effects=True, vmem_limit_bytes=56 << 20
        ),
    )(select, weigh, normed, middle, gate, up, down)


def routing(expert_ids, route_weights):
    rows_here = expert_ids.shape[0]
    z, y, x, _ = place()
    table = jnp.array(OFFSETS, jnp.int32)
    owner = (
        lax.rem(z + table[:, 0], 4) * 16 + lax.rem(y + table[:, 1], 4) * 4 + lax.rem(x + table[:, 2], 4)
    )
    target = (owner[:, None] * SLOT + jnp.arange(SLOT, dtype=jnp.int32)[None, :]).reshape(-1)
    every = jnp.arange(len(OFFSETS), dtype=jnp.int32)[None, :]
    named = [expert_ids[:, j : j + 1] == every for j in range(expert_ids.shape[1])]
    used = jnp.where(named[0] | named[1], 1.0, 0.0).astype(jnp.bfloat16)
    earlier = jnp.tril(jnp.ones((rows_here, rows_here), jnp.bfloat16), -1)
    rank = jnp.dot(earlier, used, preferred_element_type=jnp.float32)
    slots = [
        expert_ids[:, j] * SLOT + jnp.sum(jnp.where(named[j], rank, 0.0), axis=1).astype(jnp.int32)
        for j in range(expert_ids.shape[1])
    ]
    select = ((target[:, None] == slots[0][None, :]) | (target[:, None] == slots[1][None, :])).astype(
        jnp.bfloat16
    )
    weigh = sum(
        jnp.where(slots[j][:, None] == target[None, :], route_weights[:, j : j + 1], 0.0)
        for j in range(2)
    )
    high = weigh.astype(jnp.bfloat16)
    low = (weigh - high.astype(jnp.float32)).astype(jnp.bfloat16)
    return select, jnp.stack([high, low])


def body(
    stream,
    queries,
    key_rows,
    value_rows,
    out_gate,
    in_gate,
    forget_gate,
    out_proj,
    ffn_gain,
    gate_proj,
    up_proj,
    down_proj,
    expert_ids,
    route_weights,
):
    heads_here, length = in_gate.shape
    blocks = length // BLOCK

    def per_head(rows, size):
        return (
            rows.astype(jnp.float32).reshape(blocks, BLOCK, heads_here, size).transpose(2, 0, 1, 3)
        )

    query_blocks = per_head(queries, QK)
    key_blocks = per_head(key_rows, QK) * QK ** (-0.5)
    value_blocks = per_head(value_rows, V_DIM)
    input_gate = in_gate.reshape(heads_here, blocks, BLOCK)
    cumulative = jnp.cumsum(
        jax.nn.log_sigmoid(forget_gate).reshape(heads_here, blocks, BLOCK), axis=-1
    )
    closing = cumulative[..., -1]
    causal = jnp.tril(jnp.ones((BLOCK, BLOCK), dtype=bool))
    log_inner = jnp.where(
        causal,
        cumulative[..., :, None] - cumulative[..., None, :] + input_gate[..., None, :],
        -jnp.inf,
    )
    log_close = closing[..., None] - cumulative + input_gate

    def advance(carry, inputs):
        state, level, decay = carry
        key_block, value_block, close_block, last_block = inputs
        new_level = jnp.maximum(last_block + level, jnp.max(close_block, axis=-1))
        weight = jnp.exp(close_block - new_level[:, None])
        update = jnp.einsum("hl,hld,hle->hde", weight, key_block, value_block)
        new_state = state * jnp.exp(last_block + level - new_level)[:, None, None] + update
        return ((new_state, new_level, decay + last_block), (state, level, decay))

    empty = (
        jnp.zeros((heads_here, QK, V_DIM), jnp.float32),
        jnp.full((heads_here,), floor_level, jnp.float32),
        jnp.zeros((heads_here,), jnp.float32),
    )
    summary, before = lax.scan(
        advance,
        empty,
        (
            jnp.moveaxis(key_blocks, 1, 0),
            jnp.moveaxis(value_blocks, 1, 0),
            jnp.moveaxis(log_close, 1, 0),
            closing.T,
        ),
    )
    carried = prefix_by_axis(summary, SP, join_states, empty)
    anchor = join_states(
        (
            jnp.zeros((heads_here, QK, V_DIM), jnp.float32),
            jnp.zeros((heads_here,), jnp.float32),
            jnp.zeros((heads_here,), jnp.float32),
        ),
        carried,
    )
    anchor_state, anchor_level, _ = anchor
    block_states, block_levels, block_decays = before
    levels = jnp.maximum(block_decays + anchor_level[None, :], block_levels)
    states = (
        anchor_state[None] * jnp.exp(block_decays + anchor_level[None, :] - levels)[..., None, None]
        + block_states * jnp.exp(block_levels - levels)[..., None, None]
    )
    states = jnp.moveaxis(states, 0, 1)
    levels = levels.T
    log_inter = cumulative + levels[..., None]
    peak = jnp.maximum(log_inter, jnp.max(log_inner, axis=-1))
    scores = jnp.einsum("hntd,hnsd->hnts", query_blocks, key_blocks) * jnp.exp(
        log_inner - peak[..., None]
    )
    from_state = jnp.einsum("hntd,hnde->hnte", query_blocks, states)
    from_block = jnp.einsum("hnts,hnse->hnte", scores, value_blocks)
    numerator = jnp.exp(log_inter - peak)[..., None] * from_state + from_block
    numerator = numerator.transpose(1, 2, 0, 3).reshape(length, heads_here, V_DIM)
    scaled = numerator * lax.rsqrt(
        jnp.mean(numerator * numerator, axis=-1, keepdims=True) + epsilon
    )
    gated = scaled.reshape(length, heads_here * V_DIM) * jax.nn.sigmoid(
        out_gate.astype(jnp.float32)
    )
    heads_out = gated.astype(jnp.bfloat16)
    rows_here, model_width = stream.shape
    token_heads = lax.all_to_all(heads_out, "tp", split_axis=0, concat_axis=1, tiled=True)
    mix = jnp.dot(token_heads, out_proj, preferred_element_type=jnp.float32)
    middle = (stream.astype(jnp.float32) + mix).astype(jnp.bfloat16)
    middle_float = middle.astype(jnp.float32)
    normed = (
        middle_float
        * lax.rsqrt(jnp.mean(middle_float * middle_float, axis=-1, keepdims=True) + epsilon)
        * ffn_gain
    ).astype(jnp.bfloat16)
    select, weigh = routing(expert_ids, route_weights)
    return experts(select, weigh, normed, middle, gate_proj[0], up_proj[0], down_proj[0])


def solution(mesh):
    split = Mesh(mesh.devices.reshape(4, 4, 4, mesh.shape["tp"]), ("sp_0", "sp_1", "sp_2", "tp"))
    return jax.shard_map(
        body,
        mesh=split,
        in_specs=(
            P(SP_TP, None),
            P(SP, "tp"),
            P(SP, "tp"),
            P(SP, "tp"),
            P(SP, "tp"),
            P("tp", SP),
            P("tp", SP),
            P(),
            P(),
            P(SP, None, "tp"),
            P(SP, None, "tp"),
            P(SP, "tp", None),
            P(SP_TP, None),
            P(SP_TP, None),
        ),
        out_specs=P(SP_TP, None),
        check_vma=False,
    )
```

```python
import jax
import jax.numpy as jnp
from jax import lax
from jax.experimental import pallas as pl
from jax.experimental.pallas import tpu as pltpu
from jax.sharding import Mesh
from jax.sharding import PartitionSpec as P

MESH = pl.DeviceIdType.MESH
QK = 128
V_DIM = 256
SP = ("sp_0", "sp_1", "sp_2")
SP_TP = ("sp_0", "sp_1", "sp_2", "tp")


epsilon = 1e-06


OFFSETS = sorted(
    ((a, b, c) for a in range(4) for b in range(4) for c in range(4)),
    key=lambda o: sum(min(v, 4 - v) for v in o),
)
SLOT = 16
GROUP_ROWS = 256
PER_GROUP = GROUP_ROWS // SLOT


def place():
    return [lax.axis_index(axis) for axis in SP_TP]


def peer(here, offset, sign=1):
    z, y, x, core = here
    return tuple(lax.rem(p + (sign * o) % 4, 4) for p, o in zip((z, y, x), offset)) + (core,)


def experts_kernel(
    select_ref,
    weigh_ref,
    normed_ref,
    middle_ref,
    gate_ref,
    up_ref,
    down_ref,
    out_ref,
    outgoing,
    arrived,
    answers,
    returned,
    gate_full,
    up_full,
    down_full,
    hidden,
    total,
    local_sem,
    weight_send,
    weight_recv,
    send_sem,
    recv_sem,
    back_send,
    back_recv,
):
    here = place()
    other = (here[0], here[1], here[2], 1 - here[3])
    barrier = pltpu.get_barrier_semaphore()
    for offset in OFFSETS[1:]:
        pl.semaphore_signal(barrier, inc=1, device_id=peer(here, offset), device_id_type=MESH)
    pl.semaphore_signal(barrier, inc=1, device_id=other, device_id_type=MESH)
    half = gate_ref.shape[1]
    locals_ = [
        pltpu.make_async_copy(gate_ref, gate_full.at[:, pl.ds(0, half)], local_sem.at[0]),
        pltpu.make_async_copy(up_ref, up_full.at[:, pl.ds(0, half)], local_sem.at[1]),
        pltpu.make_async_copy(down_ref, down_full.at[pl.ds(0, half)], local_sem.at[2]),
    ]
    for copy in locals_:
        copy.start()

    def rows(i):
        return pl.ds(i * SLOT, SLOT)

    def group(g):
        return pl.ds(g * GROUP_ROWS, GROUP_ROWS)

    groups = len(OFFSETS) // PER_GROUP
    tile = 256

    def build(g):
        pick = select_ref[group(g), :]
        for n in range(0, outgoing.shape[1], tile):
            cols = slice(n, n + tile)
            outgoing[group(g), cols] = jnp.dot(
                pick, normed_ref[:, cols], preferred_element_type=jnp.float32
            ).astype(jnp.bfloat16)

    def send(g):
        for i in range(max(g * PER_GROUP, 1), (g + 1) * PER_GROUP):
            pltpu.make_async_remote_copy(
                src_ref=outgoing.at[rows(i)],
                dst_ref=arrived.at[rows(i)],
                send_sem=send_sem,
                recv_sem=recv_sem.at[g],
                device_id=peer(here, OFFSETS[i]),
                device_id_type=MESH,
            ).start()

    build(0)
    pl.semaphore_wait(barrier, len(OFFSETS))
    weights = [
        pltpu.make_async_remote_copy(
            src_ref=mine,
            dst_ref=theirs,
            send_sem=weight_send.at[i],
            recv_sem=weight_recv.at[i],
            device_id=other,
            device_id_type=MESH,
        )
        for i, (mine, theirs) in enumerate(
            (
                (gate_ref, gate_full.at[:, pl.ds(half, half)]),
                (up_ref, up_full.at[:, pl.ds(half, half)]),
                (down_ref, down_full.at[pl.ds(half, half)]),
            )
        )
    ]
    for g in range(1, groups):
        build(g)
        send(g - 1)
        if g == 1:
            for copy in weights:
                copy.start()
    arrived[rows(0), :] = outgoing[rows(0), :]
    send(groups - 1)

    def landed(ref, sem, first, last):
        span = pl.ds(first * SLOT, (last - first) * SLOT)
        pltpu.make_async_copy(ref.at[span], ref.at[span], sem).wait()

    for copy in locals_:
        copy.wait()
    for copy in weights:
        copy.wait_recv()
    for g in range(groups):
        landed(arrived, recv_sem.at[g], max(g * PER_GROUP, 1), (g + 1) * PER_GROUP)
        block = arrived[group(g), :]
        for n in range(0, hidden.shape[1], tile):
            cols = slice(n, n + tile)
            gates = jnp.dot(block, gate_full[:, cols], preferred_element_type=jnp.float32)
            ups = jnp.dot(block, up_full[:, cols], preferred_element_type=jnp.float32)
            hidden[:, cols] = (gates * jax.nn.sigmoid(gates) * ups).astype(jnp.bfloat16)
        for n in range(0, answers.shape[1], tile):
            cols = slice(n, n + tile)
            answers[group(g), cols] = jnp.dot(
                hidden[...], down_full[:, cols], preferred_element_type=jnp.float32
            ).astype(jnp.bfloat16)
        for i in range(max(g * PER_GROUP, 1), (g + 1) * PER_GROUP):
            pltpu.make_async_remote_copy(
                src_ref=answers.at[rows(i)],
                dst_ref=returned.at[rows(i)],
                send_sem=back_send,
                recv_sem=back_recv.at[g],
                device_id=peer(here, OFFSETS[i], -1),
                device_id_type=MESH,
            ).start()
    returned[rows(0), :] = answers[rows(0), :]
    for g in range(groups):
        landed(returned, back_recv.at[g], max(g * PER_GROUP, 1), (g + 1) * PER_GROUP)
        for n in range(0, out_ref.shape[1], tile):
            cols = slice(n, n + tile)
            part = jnp.dot(
                weigh_ref[0, :, group(g)],
                returned[group(g), cols],
                preferred_element_type=jnp.float32,
            ) + jnp.dot(
                weigh_ref[1, :, group(g)],
                returned[group(g), cols],
                preferred_element_type=jnp.float32,
            )
            before = middle_ref[:, cols].astype(jnp.float32) if g == 0 else total[:, cols]
            if g < groups - 1:
                total[:, cols] = before + part
            else:
                out_ref[:, cols] = (before + part).astype(jnp.bfloat16)
    landed(outgoing, send_sem, 1, len(OFFSETS))
    landed(answers, back_send, 1, len(OFFSETS))
    for copy in weights:
        copy.wait_send()


def experts(select, weigh, normed, middle, gate, up, down):
    rows_here, width = normed.shape
    slots = select.shape[0]
    half = gate.shape[1]
    vmem = pl.BlockSpec(memory_space=pltpu.VMEM)
    hbm = pl.BlockSpec(memory_space=pl.ANY)
    dma = pltpu.SemaphoreType.DMA
    groups = slots // GROUP_ROWS
    return pl.pallas_call(
        experts_kernel,
        out_shape=jax.ShapeDtypeStruct((rows_here, width), jnp.bfloat16),
        in_specs=[vmem] * 4 + [hbm] * 3,
        out_specs=vmem,
        scratch_shapes=[pltpu.VMEM((slots, width), jnp.bfloat16)] * 4
        + [
            pltpu.VMEM((width, 2 * half), jnp.bfloat16),
            pltpu.VMEM((width, 2 * half), jnp.bfloat16),
            pltpu.VMEM((2 * half, width), jnp.bfloat16),
            pltpu.VMEM((GROUP_ROWS, 2 * half), jnp.bfloat16),
            pltpu.VMEM((rows_here, width), jnp.float32),
            dma((3,)),
            dma((3,)),
            dma((3,)),
            dma(()),
            dma((groups,)),
            dma(()),
            dma((groups,)),
        ],
        compiler_params=pltpu.CompilerParams(
            collective_id=1, has_side_effects=True, vmem_limit_bytes=56 << 20
        ),
    )(select, weigh, normed, middle, gate, up, down)


def routing(expert_ids, route_weights):
    rows_here = expert_ids.shape[0]
    z, y, x, _ = place()
    table = jnp.array(OFFSETS, jnp.int32)
    owner = (
        lax.rem(z + table[:, 0], 4) * 16 + lax.rem(y + table[:, 1], 4) * 4 + lax.rem(x + table[:, 2], 4)
    )
    target = (owner[:, None] * SLOT + jnp.arange(SLOT, dtype=jnp.int32)[None, :]).reshape(-1)
    every = jnp.arange(len(OFFSETS), dtype=jnp.int32)[None, :]
    named = [expert_ids[:, j : j + 1] == every for j in range(expert_ids.shape[1])]
    used = jnp.where(named[0] | named[1], 1.0, 0.0).astype(jnp.bfloat16)
    earlier = jnp.tril(jnp.ones((rows_here, rows_here), jnp.bfloat16), -1)
    rank = jnp.dot(earlier, used, preferred_element_type=jnp.float32)
    slots = [
        expert_ids[:, j] * SLOT + jnp.sum(jnp.where(named[j], rank, 0.0), axis=1).astype(jnp.int32)
        for j in range(expert_ids.shape[1])
    ]
    select = ((target[:, None] == slots[0][None, :]) | (target[:, None] == slots[1][None, :])).astype(
        jnp.bfloat16
    )
    weigh = sum(
        jnp.where(slots[j][:, None] == target[None, :], route_weights[:, j : j + 1], 0.0)
        for j in range(2)
    )
    high = weigh.astype(jnp.bfloat16)
    low = (weigh - high.astype(jnp.float32)).astype(jnp.bfloat16)
    return select, jnp.stack([high, low])


def others(here, act):
    me = (here[0] * 4 + here[1]) * 4 + here[2]

    def step(k, _):
        d = lax.rem(me + k, 64)
        act(d, (d // 16, lax.rem(d // 4, 4), lax.rem(d, 4), here[3]))
        return 0

    lax.fori_loop(1, 64, step, 0)


def mixer_kernel(
    query_ref,
    key_ref,
    value_ref,
    out_gate_ref,
    in_gate_ref,
    forget_ref,
    out_ref,
    table,
    columns,
    local_num,
    local_level,
    scalars,
    all_scalars,
    pieces,
    all_pieces,
    carries,
    carried,
    outbox,
    send_sem,
    recv_sem,
):
    here = place()
    core = here[3]
    me = (here[0] * 4 + here[1]) * 4 + here[2]
    partner = (here[0], here[1], here[2], 1 - core)
    barrier = pltpu.get_barrier_semaphore()
    others(
        here,
        lambda d, dev: pl.semaphore_signal(barrier, inc=1, device_id=dev, device_id_type=MESH),
    )
    pl.semaphore_signal(barrier, inc=1, device_id=partner, device_id_type=MESH)

    length = query_ref.shape[0]
    scale = QK ** (-0.5)
    x = forget_ref[...]
    u = jnp.exp(-jnp.abs(x))
    small = u * (1.0 - u * (0.5 - u * (1.0 / 3.0 - u * 0.25)))
    decay = jnp.minimum(x, 0.0) - jnp.where(u < 0.01, small, jnp.log(1.0 + u))
    table[...] = jnp.zeros_like(table)
    table[0:2, :] = decay
    raw = table[0:8, :]
    high = raw.astype(jnp.bfloat16).astype(jnp.float32)
    middle = (raw - high).astype(jnp.bfloat16).astype(jnp.float32)
    low = raw - high - middle
    parts = jnp.concatenate([high, middle, low], axis=0).astype(jnp.bfloat16)
    before = lax.broadcasted_iota(jnp.int32, (length, length), 0)
    after = lax.broadcasted_iota(jnp.int32, (length, length), 1)
    upper = jnp.where(before <= after, 1.0, 0.0).astype(jnp.bfloat16)
    summed = jnp.dot(parts, upper, preferred_element_type=jnp.float32)
    summed = summed[0:8] + summed[8:16] + summed[16:24]
    table[0:2, :] = summed[0:2]
    table[2:4, :] = in_gate_ref[...]
    columns[...] = table[...].T
    rows_a, peaks = [], []
    for h in range(2):
        row_a = table[2 + h : 3 + h, :] - table[h : h + 1, :]
        peak = jnp.max(row_a, axis=1, keepdims=True)
        closing = table[h : h + 1, length - 1 : length]
        scalars[h : h + 1, :] = jnp.broadcast_to(closing + peak, (1, 128))
        scalars[2 + h : 3 + h, :] = jnp.broadcast_to(closing, (1, 128))
        rows_a.append(row_a)
        peaks.append(peak)
    pl.semaphore_wait(barrier, 64)

    def copy(src, dst, lane, dev):
        return pltpu.make_async_remote_copy(
            src_ref=src,
            dst_ref=dst,
            send_sem=send_sem.at[lane],
            recv_sem=recv_sem.at[lane],
            device_id=dev,
            device_id_type=MESH,
        )

    def landed(ref, sem):
        span = ref.at[pl.ds(0, 63)]
        pltpu.make_async_copy(span, span, sem).wait()

    others(here, lambda d, dev: copy(scalars, all_scalars.at[me], 0, dev).start())
    all_scalars[me] = scalars[...]
    for h in range(2):
        col_a = columns[:, 2 + h : 3 + h] - columns[:, h : h + 1]
        weight = jnp.exp(col_a - peaks[h]) * scale
        keys = (key_ref[:, h * QK : (h + 1) * QK].astype(jnp.float32) * weight).astype(jnp.bfloat16)
        state = lax.dot_general(
            keys,
            value_ref[:, h * V_DIM : (h + 1) * V_DIM],
            (((0,), (0,)), ((), ())),
            preferred_element_type=jnp.float32,
        )
        for half in range(2):
            at = h * 32 + half * 16
            pieces[at : at + 16] = state[:, half * 128 : (half + 1) * 128].reshape(16, 8, 128)
    others(here, lambda d, dev: copy(pieces.at[d], all_pieces.at[me], 1, dev).start())
    all_pieces[me] = pieces[me]

    step = 128
    for h in range(2):
        for r in range(length // step):
            n = (r + 1) * step
            rows = slice(r * step, n)
            score = lax.dot_general(
                query_ref[rows, h * QK : (h + 1) * QK],
                key_ref[0:n, h * QK : (h + 1) * QK],
                (((1,), (1,)), ((), ())),
                preferred_element_type=jnp.float32,
            )
            t = lax.broadcasted_iota(jnp.int32, (step, n), 0) + r * step
            s = lax.broadcasted_iota(jnp.int32, (step, n), 1)
            log_inner = jnp.where(s <= t, columns[rows, h : h + 1] + rows_a[h][:, 0:n], -1e30)
            level = jnp.max(log_inner, axis=1, keepdims=True)
            score = (score * scale * jnp.exp(log_inner - level)).astype(jnp.bfloat16)
            local_num[rows, h * V_DIM : (h + 1) * V_DIM] = jnp.dot(
                score, value_ref[0:n, h * V_DIM : (h + 1) * V_DIM], preferred_element_type=jnp.float32
            )
            local_level[h, rows, :] = jnp.broadcast_to(level, (step, 128))

    landed(all_scalars, recv_sem.at[0])

    def climb(s, level):
        new = jnp.maximum(all_scalars[s, 2:4, :] + level, all_scalars[s, 0:2, :])
        return jnp.where(s < me, new, level)

    anchor = lax.fori_loop(0, 64, climb, jnp.zeros((2, 128), jnp.float32))
    landed(all_pieces, recv_sem.at[1])
    head = me // 32

    def scan(s, held):
        state, level = held
        carries[s] = state
        late = all_scalars[s, pl.ds(head, 1), :]
        moved = all_scalars[s, pl.ds(2 + head, 1), :] + level
        new = jnp.maximum(moved, late)
        state = state * jnp.exp(moved - new) + all_pieces[s] * jnp.exp(late - new)
        return (state, new)

    lax.fori_loop(0, 64, scan, (jnp.zeros((8, 128), jnp.float32), jnp.zeros((1, 128), jnp.float32)))
    others(here, lambda d, dev: copy(carries.at[d], carried.at[me], 2, dev).start())
    carried[me] = carries[me]
    landed(carried, recv_sem.at[2])

    span = length // 2

    def finish(start, store):
        rows = pl.ds(pl.multiple_of(start, span), span)
        for h in range(2):
            state = jnp.concatenate(
                [
                    carried[h * 32 + half * 16 : h * 32 + (half + 1) * 16].reshape(QK, 128)
                    for half in range(2)
                ],
                axis=1,
            ).astype(jnp.bfloat16)
            wide = slice(h * V_DIM, (h + 1) * V_DIM)
            from_state = jnp.dot(
                query_ref[rows, h * QK : (h + 1) * QK], state, preferred_element_type=jnp.float32
            )
            log_inter = columns[rows, h : h + 1] + anchor[h : h + 1, 0:1]
            level = local_level[h, rows, 0:1]
            peak = jnp.maximum(log_inter, level)
            number = (
                jnp.exp(log_inter - peak) * from_state + jnp.exp(level - peak) * local_num[rows, wide]
            )
            scaled = number * lax.rsqrt(
                jnp.mean(number * number, axis=1, keepdims=True) + epsilon
            )
            gate = jax.nn.sigmoid(out_gate_ref[rows, wide].astype(jnp.float32))
            store(h, (scaled * gate).astype(jnp.bfloat16))

    def to_partner(h, value):
        outbox[:, h * V_DIM : (h + 1) * V_DIM] = value

    def to_self(h, value):
        start = pl.multiple_of(core * 2 * V_DIM + h * V_DIM, V_DIM)
        out_ref[:, pl.ds(start, V_DIM)] = value

    finish((1 - core) * span, to_partner)
    mine = pl.ds(pl.multiple_of(core * 2 * V_DIM, 2 * V_DIM), 2 * V_DIM)
    swap = copy(outbox, out_ref.at[:, mine], 3, partner)
    swap.start()
    finish(core * span, to_self)
    swap.wait()
    for ref, lane in ((all_scalars, 0), (all_pieces, 1), (carried, 2)):
        landed(ref, send_sem.at[lane])


def mixer(queries, key_rows, value_rows, out_gate, in_gate, forget_gate):
    length = queries.shape[0]
    vmem = pl.BlockSpec(memory_space=pltpu.VMEM)
    f32 = jnp.float32
    return pl.pallas_call(
        mixer_kernel,
        out_shape=jax.ShapeDtypeStruct((length // 2, 4 * V_DIM), jnp.bfloat16),
        in_specs=[vmem] * 6,
        out_specs=vmem,
        scratch_shapes=[
            pltpu.VMEM((128, length), f32),
            pltpu.VMEM((length, 128), f32),
            pltpu.VMEM((length, 2 * V_DIM), f32),
            pltpu.VMEM((2, length, 128), f32),
            pltpu.VMEM((4, 128), f32),
            pltpu.VMEM((64, 4, 128), f32),
        ]
        + [pltpu.VMEM((64, 8, 128), f32)] * 4
        + [
            pltpu.VMEM((length // 2, 2 * V_DIM), jnp.bfloat16),
            pltpu.SemaphoreType.DMA((4,)),
            pltpu.SemaphoreType.DMA((4,)),
        ],
        compiler_params=pltpu.CompilerParams(
            collective_id=0, has_side_effects=True, vmem_limit_bytes=32 << 20
        ),
    )(queries, key_rows, value_rows, out_gate, in_gate, forget_gate)


def body(
    stream,
    queries,
    key_rows,
    value_rows,
    out_gate,
    in_gate,
    forget_gate,
    out_proj,
    ffn_gain,
    gate_proj,
    up_proj,
    down_proj,
    expert_ids,
    route_weights,
):
    token_heads = mixer(queries, key_rows, value_rows, out_gate, in_gate, forget_gate)
    mix = jnp.dot(token_heads, out_proj, preferred_element_type=jnp.float32)
    middle = (stream.astype(jnp.float32) + mix).astype(jnp.bfloat16)
    middle_float = middle.astype(jnp.float32)
    normed = (
        middle_float
        * lax.rsqrt(jnp.mean(middle_float * middle_float, axis=-1, keepdims=True) + epsilon)
        * ffn_gain
    ).astype(jnp.bfloat16)
    select, weigh = routing(expert_ids, route_weights)
    return experts(select, weigh, normed, middle, gate_proj[0], up_proj[0], down_proj[0])


def solution(mesh):
    split = Mesh(mesh.devices.reshape(4, 4, 4, mesh.shape["tp"]), ("sp_0", "sp_1", "sp_2", "tp"))
    return jax.shard_map(
        body,
        mesh=split,
        in_specs=(
            P(SP_TP, None),
            P(SP, "tp"),
            P(SP, "tp"),
            P(SP, "tp"),
            P(SP, "tp"),
            P("tp", SP),
            P("tp", SP),
            P(),
            P(),
            P(SP, None, "tp"),
            P(SP, None, "tp"),
            P(SP, "tp", None),
            P(SP_TP, None),
            P(SP_TP, None),
        ),
        out_specs=P(SP_TP, None),
        check_vma=False,
    )
```

```python
import jax
import jax.numpy as jnp
from jax import lax
from jax.experimental import pallas as pl
from jax.experimental.pallas import tpu as pltpu
from jax.sharding import Mesh
from jax.sharding import PartitionSpec as P

MESH = pl.DeviceIdType.MESH
QK = 128
V_DIM = 256
SP = ("sp_0", "sp_1", "sp_2")
SP_TP = ("sp_0", "sp_1", "sp_2", "tp")
SLOT = 16
GROUP_ROWS = 256
PER_GROUP = GROUP_ROWS // SLOT
TILE = 256
epsilon = 1e-06
F32 = jnp.float32
BF16 = jnp.bfloat16


def offsets_by_orbit():
    cube = [(a, b, c) for a in range(4) for b in range(4) for c in range(4)]
    seen, orbits = {(0, 0, 0)}, []
    for o in sorted(cube, key=lambda o: sum(min(v, 4 - v) for v in o)):
        orbit = []
        for turn in range(3):
            turned = o[turn:] + o[:turn]
            for p in (turned, tuple(-v % 4 for v in turned)):
                if p not in seen:
                    seen.add(p)
                    orbit.append(p)
        if orbit:
            orbits.append(orbit)
    order = [(0, 0, 0)]
    while orbits:
        order += orbits.pop(0)
        if orbits:
            order += orbits.pop()
    return order


OFFSETS = offsets_by_orbit()
GROUPS = len(OFFSETS) // PER_GROUP


def place():
    return [lax.axis_index(axis) for axis in SP_TP]


def peer(here, offset, sign=1):
    z, y, x, core = here
    return tuple(lax.rem(p + (sign * o) % 4, 4) for p, o in zip((z, y, x), offset)) + (core,)


def index_of(device):
    return (device[0] * 4 + device[1]) * 4 + device[2]


def others(here, act):
    me = index_of(here)

    def step(k, _):
        d = lax.rem(me + k, 64)
        act(d, (d // 16, lax.rem(d // 4, 4), lax.rem(d, 4), here[3]))
        return 0

    lax.fori_loop(1, 64, step, 0)


def route(ids_ref, routes_ref, pairs, ranks, shares, select_ref, weigh_ref, here, loads):
    loads["ids"].wait()
    loads["routes"].wait()
    pairs[...] = jnp.zeros_like(pairs)
    pairs[:, 0:2] = ids_ref[...].astype(F32)
    pairs[:, 2:4] = routes_ref[...]
    turned = pairs[...].T
    tokens = turned.shape[1]
    expert = lax.broadcasted_iota(jnp.int32, (len(OFFSETS), tokens), 0).astype(F32)
    first, second = (turned[j : j + 1, :] == expert for j in range(2))
    used = jnp.where(first | second, 1.0, 0.0)
    earlier = lax.broadcasted_iota(jnp.int32, (tokens, tokens), 0)
    later = lax.broadcasted_iota(jnp.int32, (tokens, tokens), 1)
    upper = jnp.where(earlier < later, 1.0, 0.0).astype(BF16)
    rank = jnp.dot(used.astype(BF16), upper, preferred_element_type=F32)
    ranks[...] = jnp.where(first | second, rank, -1.0)
    shares[...] = jnp.where(first, turned[2:3, :], 0.0) + jnp.where(second, turned[3:4, :], 0.0)
    slot = lax.broadcasted_iota(jnp.int32, (SLOT, tokens), 0).astype(F32)
    for g in range(GROUPS):
        weights = []
        for i in range(g * PER_GROUP, (g + 1) * PER_GROUP):
            owner = pl.ds(index_of(peer(here, OFFSETS[i])), 1)
            chosen = ranks[owner, :] == slot
            select_ref[pl.ds(i * SLOT, SLOT), :] = jnp.where(chosen, 1.0, 0.0).astype(BF16)
            weights.append(jnp.where(chosen, shares[owner, :], 0.0))
        weigh = jnp.concatenate(weights, axis=0).T
        high = weigh.astype(BF16)
        cols = slice(g * GROUP_ROWS, (g + 1) * GROUP_ROWS)
        weigh_ref[0, :, cols] = high
        weigh_ref[1, :, cols] = (weigh - high.astype(F32)).astype(BF16)


def layer_kernel(
    stream_hbm,
    query_hbm,
    key_hbm,
    value_hbm,
    out_gate_hbm,
    in_gate_hbm,
    forget_hbm,
    out_proj_hbm,
    gain_hbm,
    gate_ref,
    up_ref,
    down_ref,
    ids_hbm,
    routes_hbm,
    out_ref,
    stream_ref,
    query_ref,
    key_ref,
    value_ref,
    out_gate_ref,
    in_gate_ref,
    forget_ref,
    out_proj_ref,
    gain_ref,
    ids_ref,
    routes_ref,
    table,
    columns,
    local_num,
    local_level,
    scalars,
    all_scalars,
    pieces,
    all_pieces,
    carries,
    carried,
    outbox,
    heads,
    pairs,
    ranks,
    shares,
    select_ref,
    weigh_ref,
    middle_ref,
    normed_ref,
    outgoing,
    arrived,
    answers,
    returned,
    gate_full,
    up_full,
    down_full,
    hidden,
    total,
    load_sem,
    send_sem,
    recv_sem,
    weight_send,
    weight_recv,
    rows_send,
    rows_recv,
    back_send,
    back_recv,
):
    here = place()
    core = here[3]
    me = index_of(here)
    partner = (here[0], here[1], here[2], 1 - core)
    units = gate_ref.shape[1]
    loads = {}
    for name, src, dst in (
        ("forget", forget_hbm, forget_ref),
        ("in", in_gate_hbm, in_gate_ref),
        ("key", key_hbm, key_ref),
        ("value", value_hbm, value_ref),
        ("query", query_hbm, query_ref),
        ("ids", ids_hbm, ids_ref),
        ("routes", routes_hbm, routes_ref),
        ("out_gate", out_gate_hbm, out_gate_ref),
        ("out_proj", out_proj_hbm, out_proj_ref),
        ("stream", stream_hbm, stream_ref),
        ("gain", gain_hbm, gain_ref),
        ("gate", gate_ref, gate_full.at[:, pl.ds(0, units)]),
        ("up", up_ref, up_full.at[:, pl.ds(0, units)]),
        ("down", down_ref, down_full.at[pl.ds(0, units)]),
    ):
        loads[name] = pltpu.make_async_copy(src, dst, load_sem.at[len(loads)])
        loads[name].start()
    barrier = pltpu.get_barrier_semaphore()
    others(
        here,
        lambda d, dev: pl.semaphore_signal(barrier, inc=1, device_id=dev, device_id_type=MESH),
    )
    pl.semaphore_signal(barrier, inc=1, device_id=partner, device_id_type=MESH)

    length = query_ref.shape[0]
    scale = QK ** (-0.5)
    loads["forget"].wait()
    loads["in"].wait()
    x = forget_ref[...]
    u = jnp.exp(-jnp.abs(x))
    small = u * (1.0 - u * (0.5 - u * (1.0 / 3.0 - u * 0.25)))
    decay = jnp.minimum(x, 0.0) - jnp.where(u < 0.01, small, jnp.log(1.0 + u))
    table[...] = jnp.zeros_like(table)
    table[0:2, :] = decay
    raw = table[0:8, :]
    high = raw.astype(jnp.bfloat16).astype(jnp.float32)
    mid = (raw - high).astype(jnp.bfloat16).astype(jnp.float32)
    low = raw - high - mid
    parts = jnp.concatenate([high, mid, low], axis=0).astype(jnp.bfloat16)
    before = lax.broadcasted_iota(jnp.int32, (length, length), 0)
    after = lax.broadcasted_iota(jnp.int32, (length, length), 1)
    upper = jnp.where(before <= after, 1.0, 0.0).astype(jnp.bfloat16)
    summed = jnp.dot(parts, upper, preferred_element_type=jnp.float32)
    summed = summed[0:8] + summed[8:16] + summed[16:24]
    table[0:2, :] = summed[0:2]
    table[2:4, :] = in_gate_ref[...]
    columns[...] = table[...].T
    rows_a, peaks = [], []
    for h in range(2):
        row_a = table[2 + h : 3 + h, :] - table[h : h + 1, :]
        peak = jnp.max(row_a, axis=1, keepdims=True)
        closing = table[h : h + 1, length - 1 : length]
        scalars[h : h + 1, :] = jnp.broadcast_to(closing + peak, (1, 128))
        scalars[2 + h : 3 + h, :] = jnp.broadcast_to(closing, (1, 128))
        rows_a.append(row_a)
        peaks.append(peak)
    pl.semaphore_wait(barrier, 64)

    def copy(src, dst, lane, dev):
        return pltpu.make_async_remote_copy(
            src_ref=src,
            dst_ref=dst,
            send_sem=send_sem.at[lane],
            recv_sem=recv_sem.at[lane],
            device_id=dev,
            device_id_type=MESH,
        )

    def landed(ref, sem):
        span = ref.at[pl.ds(0, 63)]
        pltpu.make_async_copy(span, span, sem).wait()

    others(here, lambda d, dev: copy(scalars, all_scalars.at[me], 0, dev).start())
    all_scalars[me] = scalars[...]
    loads["key"].wait()
    loads["value"].wait()
    for h in range(2):
        col_a = columns[:, 2 + h : 3 + h] - columns[:, h : h + 1]
        weight = jnp.exp(col_a - peaks[h]) * scale
        keys = (key_ref[:, h * QK : (h + 1) * QK].astype(jnp.float32) * weight).astype(jnp.bfloat16)
        state = lax.dot_general(
            keys,
            value_ref[:, h * V_DIM : (h + 1) * V_DIM],
            (((0,), (0,)), ((), ())),
            preferred_element_type=jnp.float32,
        )
        for half in range(2):
            at = h * 32 + half * 16
            pieces[at : at + 16] = state[:, half * 128 : (half + 1) * 128].reshape(16, 8, 128)
    others(here, lambda d, dev: copy(pieces.at[d], all_pieces.at[me], 1, dev).start())
    all_pieces[me] = pieces[me]

    loads["query"].wait()
    step = 128
    for h in range(2):
        for r in range(length // step):
            n = (r + 1) * step
            rows = slice(r * step, n)
            score = lax.dot_general(
                query_ref[rows, h * QK : (h + 1) * QK],
                key_ref[0:n, h * QK : (h + 1) * QK],
                (((1,), (1,)), ((), ())),
                preferred_element_type=jnp.float32,
            )
            t = lax.broadcasted_iota(jnp.int32, (step, n), 0) + r * step
            s = lax.broadcasted_iota(jnp.int32, (step, n), 1)
            log_inner = jnp.where(s <= t, columns[rows, h : h + 1] + rows_a[h][:, 0:n], -1e30)
            level = jnp.max(log_inner, axis=1, keepdims=True)
            score = (score * scale * jnp.exp(log_inner - level)).astype(jnp.bfloat16)
            local_num[rows, h * V_DIM : (h + 1) * V_DIM] = jnp.dot(
                score, value_ref[0:n, h * V_DIM : (h + 1) * V_DIM], preferred_element_type=jnp.float32
            )
            local_level[h, rows, :] = jnp.broadcast_to(level, (step, 128))

    landed(all_scalars, recv_sem.at[0])

    def climb(s, level):
        new = jnp.maximum(all_scalars[s, 2:4, :] + level, all_scalars[s, 0:2, :])
        return jnp.where(s < me, new, level)

    anchor = lax.fori_loop(0, 64, climb, jnp.zeros((2, 128), jnp.float32))
    landed(all_pieces, recv_sem.at[1])
    head = me // 32

    def scan(s, held):
        state, level = held
        carries[s] = state
        late = all_scalars[s, pl.ds(head, 1), :]
        moved = all_scalars[s, pl.ds(2 + head, 1), :] + level
        new = jnp.maximum(moved, late)
        state = state * jnp.exp(moved - new) + all_pieces[s] * jnp.exp(late - new)
        return (state, new)

    lax.fori_loop(0, 64, scan, (jnp.zeros((8, 128), jnp.float32), jnp.zeros((1, 128), jnp.float32)))
    others(here, lambda d, dev: copy(carries.at[d], carried.at[me], 2, dev).start())
    carried[me] = carries[me]
    route(ids_ref, routes_ref, pairs, ranks, shares, select_ref, weigh_ref, here, loads)
    landed(carried, recv_sem.at[2])

    span = length // 2

    def finish(start, store):
        rows = pl.ds(pl.multiple_of(start, span), span)
        for h in range(2):
            state = jnp.concatenate(
                [
                    carried[h * 32 + half * 16 : h * 32 + (half + 1) * 16].reshape(QK, 128)
                    for half in range(2)
                ],
                axis=1,
            ).astype(jnp.bfloat16)
            wide = slice(h * V_DIM, (h + 1) * V_DIM)
            from_state = jnp.dot(
                query_ref[rows, h * QK : (h + 1) * QK], state, preferred_element_type=jnp.float32
            )
            log_inter = columns[rows, h : h + 1] + anchor[h : h + 1, 0:1]
            level = local_level[h, rows, 0:1]
            peak = jnp.maximum(log_inter, level)
            number = (
                jnp.exp(log_inter - peak) * from_state + jnp.exp(level - peak) * local_num[rows, wide]
            )
            scaled = number * lax.rsqrt(
                jnp.mean(number * number, axis=1, keepdims=True) + epsilon
            )
            gate = jax.nn.sigmoid(out_gate_ref[rows, wide].astype(jnp.float32))
            store(h, (scaled * gate).astype(jnp.bfloat16))

    def to_partner(h, value):
        outbox[:, h * V_DIM : (h + 1) * V_DIM] = value

    def to_self(h, value):
        start = pl.multiple_of(core * 2 * V_DIM + h * V_DIM, V_DIM)
        heads[:, pl.ds(start, V_DIM)] = value

    loads["out_gate"].wait()
    finish((1 - core) * span, to_partner)
    mine = pl.ds(pl.multiple_of(core * 2 * V_DIM, 2 * V_DIM), 2 * V_DIM)
    swap = copy(outbox, heads.at[:, mine], 3, partner)
    swap.start()
    weights = [
        pltpu.make_async_remote_copy(
            src_ref=mine_,
            dst_ref=theirs,
            send_sem=weight_send.at[i],
            recv_sem=weight_recv.at[i],
            device_id=partner,
            device_id_type=MESH,
        )
        for i, (mine_, theirs) in enumerate(
            (
                (gate_ref, gate_full.at[:, pl.ds(units, units)]),
                (up_ref, up_full.at[:, pl.ds(units, units)]),
                (down_ref, down_full.at[pl.ds(units, units)]),
            )
        )
    ]
    for weight in weights:
        weight.start()
    finish(core * span, to_self)
    swap.wait()
    loads["out_proj"].wait()
    loads["stream"].wait()
    loads["gain"].wait()
    width = stream_ref.shape[1]
    tiles = [slice(n, n + TILE) for n in range(0, width, TILE)]
    squares = jnp.zeros((stream_ref.shape[0], 1), F32)
    for cols in tiles:
        mix = jnp.dot(heads[...], out_proj_ref[:, cols], preferred_element_type=F32)
        both = (stream_ref[:, cols].astype(F32) + mix).astype(BF16)
        middle_ref[:, cols] = both
        both = both.astype(F32)
        squares = squares + jnp.sum(both * both, axis=1, keepdims=True)
    factor = lax.rsqrt(squares / width + epsilon)
    for cols in tiles:
        normed_ref[:, cols] = (middle_ref[:, cols].astype(F32) * factor * gain_ref[:, cols]).astype(BF16)

    def rows(i):
        return pl.ds(i * SLOT, SLOT)

    def group(g):
        return pl.ds(g * GROUP_ROWS, GROUP_ROWS)

    def members(g):
        return range(max(g * PER_GROUP, 1), (g + 1) * PER_GROUP)

    def build(g):
        pick = select_ref[group(g), :]
        for cols in tiles:
            outgoing[group(g), cols] = jnp.dot(
                pick, normed_ref[:, cols], preferred_element_type=F32
            ).astype(BF16)

    def send(g):
        for i in members(g):
            pltpu.make_async_remote_copy(
                src_ref=outgoing.at[rows(i)],
                dst_ref=arrived.at[rows(i)],
                send_sem=rows_send,
                recv_sem=rows_recv.at[g],
                device_id=peer(here, OFFSETS[i]),
                device_id_type=MESH,
            ).start()

    build(0)
    for g in range(1, GROUPS):
        send(g - 1)
        build(g)
    arrived[rows(0), :] = outgoing[rows(0), :]
    send(GROUPS - 1)

    def all_in(ref, sem, first, last):
        span = ref.at[pl.ds(first * SLOT, (last - first) * SLOT)]
        pltpu.make_async_copy(span, span, sem).wait()

    for name in ("gate", "up", "down"):
        loads[name].wait()
    for weight in weights:
        weight.wait_recv()
    for g in range(GROUPS):
        all_in(arrived, rows_recv.at[g], members(g)[0], members(g)[-1] + 1)
        block = arrived[group(g), :]
        for n in range(0, hidden.shape[1], TILE):
            cols = slice(n, n + TILE)
            gates = jnp.dot(block, gate_full[:, cols], preferred_element_type=F32)
            ups = jnp.dot(block, up_full[:, cols], preferred_element_type=F32)
            hidden[:, cols] = (gates * jax.nn.sigmoid(gates) * ups).astype(BF16)
        for cols in tiles:
            answers[group(g), cols] = jnp.dot(
                hidden[...], down_full[:, cols], preferred_element_type=F32
            ).astype(BF16)
        for i in members(g):
            pltpu.make_async_remote_copy(
                src_ref=answers.at[rows(i)],
                dst_ref=returned.at[rows(i)],
                send_sem=back_send,
                recv_sem=back_recv.at[g],
                device_id=peer(here, OFFSETS[i], -1),
                device_id_type=MESH,
            ).start()
    returned[rows(0), :] = answers[rows(0), :]
    for g in range(GROUPS):
        all_in(returned, back_recv.at[g], members(g)[0], members(g)[-1] + 1)
        for cols in tiles:
            part = jnp.dot(
                weigh_ref[0, :, group(g)], returned[group(g), cols], preferred_element_type=F32
            ) + jnp.dot(
                weigh_ref[1, :, group(g)], returned[group(g), cols], preferred_element_type=F32
            )
            before = middle_ref[:, cols].astype(F32) if g == 0 else total[:, cols]
            if g < GROUPS - 1:
                total[:, cols] = before + part
            else:
                out_ref[:, cols] = (before + part).astype(out_ref.dtype)
    all_in(outgoing, rows_send, 1, len(OFFSETS))
    all_in(answers, back_send, 1, len(OFFSETS))
    for weight in weights:
        weight.wait_send()
    for ref, lane in ((all_scalars, 0), (all_pieces, 1), (carried, 2)):
        landed(ref, send_sem.at[lane])


def body(*arrays):
    (
        stream,
        queries,
        key_rows,
        value_rows,
        out_gate,
        in_gate,
        forget_gate,
        out_proj,
        ffn_gain,
        gate_proj,
        up_proj,
        down_proj,
        expert_ids,
        route_weights,
    ) = arrays
    rows_here, width = stream.shape
    length = queries.shape[0]
    half = gate_proj.shape[2]
    slots = len(OFFSETS) * SLOT
    gain = ffn_gain.reshape(1, width)
    loaded = [
        stream,
        queries,
        key_rows,
        value_rows,
        out_gate,
        in_gate,
        forget_gate,
        out_proj,
        gain,
        expert_ids,
        route_weights,
    ]
    vmem, dma = pltpu.VMEM, pltpu.SemaphoreType.DMA
    return pl.pallas_call(
        layer_kernel,
        out_shape=jax.ShapeDtypeStruct((rows_here, width), BF16),
        in_specs=[pl.BlockSpec(memory_space=pl.ANY)] * 14,
        out_specs=pl.BlockSpec(memory_space=pltpu.VMEM),
        scratch_shapes=[vmem(a.shape, a.dtype) for a in loaded]
        + [
            vmem((128, length), F32),
            vmem((length, 128), F32),
            vmem((length, 2 * V_DIM), F32),
            vmem((2, length, 128), F32),
            vmem((4, 128), F32),
            vmem((64, 4, 128), F32),
        ]
        + [vmem((64, 8, 128), F32)] * 4
        + [
            vmem((rows_here, 2 * V_DIM), BF16),
            vmem((rows_here, 4 * V_DIM), BF16),
            vmem((rows_here, 128), F32),
            vmem((len(OFFSETS), rows_here), F32),
            vmem((len(OFFSETS), rows_here), F32),
            vmem((slots, rows_here), BF16),
            vmem((2, rows_here, slots), BF16),
            vmem((rows_here, width), BF16),
            vmem((rows_here, width), BF16),
        ]
        + [vmem((slots, width), BF16)] * 4
        + [
            vmem((width, 2 * half), BF16),
            vmem((width, 2 * half), BF16),
            vmem((2 * half, width), BF16),
            vmem((GROUP_ROWS, 2 * half), BF16),
            vmem((rows_here, width), F32),
            dma((14,)),
            dma((4,)),
            dma((4,)),
            dma((3,)),
            dma((3,)),
            dma(()),
            dma((GROUPS,)),
            dma(()),
            dma((GROUPS,)),
        ],
        compiler_params=pltpu.CompilerParams(
            collective_id=0, has_side_effects=True, vmem_limit_bytes=62 << 20
        ),
    )(
        stream,
        queries,
        key_rows,
        value_rows,
        out_gate,
        in_gate,
        forget_gate,
        out_proj,
        gain,
        gate_proj[0],
        up_proj[0],
        down_proj[0],
        expert_ids,
        route_weights,
    )


def solution(mesh):
    split = Mesh(mesh.devices.reshape(4, 4, 4, mesh.shape["tp"]), ("sp_0", "sp_1", "sp_2", "tp"))
    return jax.shard_map(
        body,
        mesh=split,
        in_specs=(
            P(SP_TP, None),
            P(SP, "tp"),
            P(SP, "tp"),
            P(SP, "tp"),
            P(SP, "tp"),
            P("tp", SP),
            P("tp", SP),
            P(),
            P(),
            P(SP, None, "tp"),
            P(SP, None, "tp"),
            P(SP, "tp", None),
            P(SP_TP, None),
            P(SP_TP, None),
        ),
        out_specs=P(SP_TP, None),
        check_vma=False,
    )
```

```python
import jax
import jax.numpy as jnp
from jax import lax
from jax.experimental import pallas as pl
from jax.experimental.pallas import tpu as pltpu
from jax.sharding import Mesh
from jax.sharding import PartitionSpec as P

MESH = pl.DeviceIdType.MESH
QK = 128
V_DIM = 256
SP = ("sp_0", "sp_1", "sp_2")
SP_TP = ("sp_0", "sp_1", "sp_2", "tp")
SLOT = 16
GROUP_ROWS = 256
PER_GROUP = GROUP_ROWS // SLOT
TILE = 256
epsilon = 1e-06
F32 = jnp.float32
BF16 = jnp.bfloat16


def offsets_by_orbit():
    cube = [(a, b, c) for a in range(4) for b in range(4) for c in range(4)]
    seen, orbits = {(0, 0, 0)}, []
    for o in sorted(cube, key=lambda o: sum(min(v, 4 - v) for v in o)):
        orbit = []
        for turn in range(3):
            turned = o[turn:] + o[:turn]
            for p in (turned, tuple(-v % 4 for v in turned)):
                if p not in seen:
                    seen.add(p)
                    orbit.append(p)
        if orbit:
            orbits.append(orbit)
    order = [(0, 0, 0)]
    while orbits:
        order += orbits.pop(0)
        if orbits:
            order += orbits.pop()
    return order


OFFSETS = offsets_by_orbit()
GROUPS = len(OFFSETS) // PER_GROUP


def place():
    return [lax.axis_index(axis) for axis in SP_TP]


def peer(here, offset, sign=1):
    z, y, x, core = here
    return tuple(lax.rem(p + (sign * o) % 4, 4) for p, o in zip((z, y, x), offset)) + (core,)


def index_of(device):
    return (device[0] * 4 + device[1]) * 4 + device[2]


FAR_FIRST = sorted(OFFSETS[1:], key=lambda o: -sum(min(v, 4 - v) for v in o))


def others(here, act):
    for offset in FAR_FIRST:
        device = peer(here, offset)
        act(index_of(device), device)


def route(ids_ref, routes_ref, ranks, shares, select_ref, weigh_ref, here, loads):
    loads["ids"].wait()
    loads["routes"].wait()
    named = ids_ref[...].astype(F32)
    tokens = named.shape[1]
    expert = lax.broadcasted_iota(jnp.int32, (len(OFFSETS), tokens), 0).astype(F32)
    first, second = (named[j : j + 1, :] == expert for j in range(2))
    used = jnp.where(first | second, 1.0, 0.0)
    earlier = lax.broadcasted_iota(jnp.int32, (tokens, tokens), 0)
    later = lax.broadcasted_iota(jnp.int32, (tokens, tokens), 1)
    upper = jnp.where(earlier < later, 1.0, 0.0).astype(BF16)
    rank = jnp.dot(used.astype(BF16), upper, preferred_element_type=F32)
    ranks[...] = jnp.where(first | second, rank, -1.0)
    shares[...] = jnp.where(first, routes_ref[0:1, :], 0.0) + jnp.where(second, routes_ref[1:2, :], 0.0)
    slot = lax.broadcasted_iota(jnp.int32, (SLOT, tokens), 0).astype(F32)
    for g in range(GROUPS):
        weights = []
        for i in range(g * PER_GROUP, (g + 1) * PER_GROUP):
            owner = pl.ds(index_of(peer(here, OFFSETS[i])), 1)
            chosen = ranks[owner, :] == slot
            select_ref[pl.ds(i * SLOT, SLOT), :] = jnp.where(chosen, 1.0, 0.0).astype(BF16)
            weights.append(jnp.where(chosen, shares[owner, :], 0.0))
        weigh = jnp.concatenate(weights, axis=0).T
        high = weigh.astype(BF16)
        cols = slice(g * GROUP_ROWS, (g + 1) * GROUP_ROWS)
        weigh_ref[0, :, cols] = high
        weigh_ref[1, :, cols] = (weigh - high.astype(F32)).astype(BF16)


def layer_kernel(
    stream_hbm,
    query_hbm,
    key_hbm,
    value_hbm,
    out_gate_hbm,
    in_gate_hbm,
    forget_hbm,
    out_proj_hbm,
    gain_hbm,
    gate_ref,
    up_ref,
    down_ref,
    ids_hbm,
    routes_hbm,
    out_ref,
    stream_ref,
    query_ref,
    key_ref,
    value_ref,
    out_gate_ref,
    in_gate_ref,
    forget_ref,
    out_proj_ref,
    gain_ref,
    ids_ref,
    routes_ref,
    table,
    columns,
    local_num,
    local_level,
    scalars,
    all_scalars,
    pieces,
    all_pieces,
    carries,
    carried,
    outbox,
    heads,
    ranks,
    shares,
    select_ref,
    weigh_ref,
    middle_ref,
    normed_ref,
    outgoing,
    arrived,
    answers,
    returned,
    gate_full,
    up_full,
    down_full,
    hidden,
    total,
    load_sem,
    send_sem,
    recv_sem,
    weight_send,
    weight_recv,
    rows_send,
    rows_recv,
    back_send,
    back_recv,
):
    here = place()
    core = here[3]
    me = index_of(here)
    partner = (here[0], here[1], here[2], 1 - core)
    units = gate_ref.shape[1]
    barrier = pltpu.get_barrier_semaphore()
    others(
        here,
        lambda d, dev: pl.semaphore_signal(barrier, inc=1, device_id=dev, device_id_type=MESH),
    )
    pl.semaphore_signal(barrier, inc=1, device_id=partner, device_id_type=MESH)
    loads = {}
    for name, src, dst in (
        ("forget", forget_hbm, forget_ref),
        ("in", in_gate_hbm, in_gate_ref),
        ("key", key_hbm, key_ref),
        ("value", value_hbm, value_ref),
        ("query", query_hbm, query_ref),
        ("ids", ids_hbm, ids_ref),
        ("routes", routes_hbm, routes_ref),
        ("out_gate", out_gate_hbm, out_gate_ref),
        ("out_proj", out_proj_hbm, out_proj_ref),
        ("stream", stream_hbm, stream_ref),
        ("gain", gain_hbm, gain_ref),
        ("gate", gate_ref, gate_full.at[:, pl.ds(0, units)]),
        ("up", up_ref, up_full.at[:, pl.ds(0, units)]),
        ("down", down_ref, down_full.at[pl.ds(0, units)]),
    ):
        loads[name] = pltpu.make_async_copy(src, dst, load_sem.at[len(loads)])
        loads[name].start()

    length = query_ref.shape[0]
    scale = QK ** (-0.5)
    loads["forget"].wait()
    loads["in"].wait()
    x = forget_ref[...]
    u = jnp.exp(-jnp.abs(x))
    small = u * (1.0 - u * (0.5 - u * (1.0 / 3.0 - u * 0.25)))
    decay = jnp.minimum(x, 0.0) - jnp.where(u < 0.01, small, jnp.log(1.0 + u))
    table[...] = jnp.zeros_like(table)
    table[0:2, :] = decay
    raw = table[0:8, :]
    high = raw.astype(jnp.bfloat16).astype(jnp.float32)
    mid = (raw - high).astype(jnp.bfloat16).astype(jnp.float32)
    low = raw - high - mid
    parts = jnp.concatenate([high, mid, low], axis=0).astype(jnp.bfloat16)
    before = lax.broadcasted_iota(jnp.int32, (length, length), 0)
    after = lax.broadcasted_iota(jnp.int32, (length, length), 1)
    upper = jnp.where(before <= after, 1.0, 0.0).astype(jnp.bfloat16)
    summed = jnp.dot(parts, upper, preferred_element_type=jnp.float32)
    summed = summed[0:8] + summed[8:16] + summed[16:24]
    table[0:2, :] = summed[0:2]
    table[2:4, :] = in_gate_ref[...]
    columns[...] = table[...].T
    rows_a, peaks = [], []
    for h in range(2):
        row_a = table[2 + h : 3 + h, :] - table[h : h + 1, :]
        peak = jnp.max(row_a, axis=1, keepdims=True)
        closing = table[h : h + 1, length - 1 : length]
        scalars[h : h + 1, :] = jnp.broadcast_to(closing + peak, (1, 128))
        scalars[2 + h : 3 + h, :] = jnp.broadcast_to(closing, (1, 128))
        rows_a.append(row_a)
        peaks.append(peak)
    loads["key"].wait()
    loads["value"].wait()
    for h in range(2):
        col_a = columns[:, 2 + h : 3 + h] - columns[:, h : h + 1]
        weight = jnp.exp(col_a - peaks[h]) * scale
        keys = (key_ref[:, h * QK : (h + 1) * QK].astype(jnp.float32) * weight).astype(jnp.bfloat16)
        state = lax.dot_general(
            keys,
            value_ref[:, h * V_DIM : (h + 1) * V_DIM],
            (((0,), (0,)), ((), ())),
            preferred_element_type=jnp.float32,
        )
        for half in range(2):
            at = h * 32 + half * 16
            pieces[at : at + 16] = state[:, half * 128 : (half + 1) * 128].reshape(16, 8, 128)
    pl.semaphore_wait(barrier, 64)

    def copy(src, dst, lane, dev):
        return pltpu.make_async_remote_copy(
            src_ref=src,
            dst_ref=dst,
            send_sem=send_sem.at[lane],
            recv_sem=recv_sem.at[lane],
            device_id=dev,
            device_id_type=MESH,
        )

    def landed(ref, sem):
        span = ref.at[pl.ds(0, 63)]
        pltpu.make_async_copy(span, span, sem).wait()

    def spread(d, dev):
        copy(scalars, all_scalars.at[me], 0, dev).start()
        copy(pieces.at[d], all_pieces.at[me], 1, dev).start()

    others(here, spread)
    all_scalars[me] = scalars[...]
    all_pieces[me] = pieces[me]

    loads["query"].wait()
    step = 128
    for h in range(2):
        for r in range(length // step):
            n = (r + 1) * step
            rows = slice(r * step, n)
            score = lax.dot_general(
                query_ref[rows, h * QK : (h + 1) * QK],
                key_ref[0:n, h * QK : (h + 1) * QK],
                (((1,), (1,)), ((), ())),
                preferred_element_type=jnp.float32,
            )
            t = lax.broadcasted_iota(jnp.int32, (step, n), 0) + r * step
            s = lax.broadcasted_iota(jnp.int32, (step, n), 1)
            log_inner = jnp.where(s <= t, columns[rows, h : h + 1] + rows_a[h][:, 0:n], -1e30)
            level = jnp.max(log_inner, axis=1, keepdims=True)
            score = (score * scale * jnp.exp(log_inner - level)).astype(jnp.bfloat16)
            local_num[rows, h * V_DIM : (h + 1) * V_DIM] = jnp.dot(
                score, value_ref[0:n, h * V_DIM : (h + 1) * V_DIM], preferred_element_type=jnp.float32
            )
            local_level[h, rows, :] = jnp.broadcast_to(level, (step, 128))

    route(ids_ref, routes_ref, ranks, shares, select_ref, weigh_ref, here, loads)
    landed(all_scalars, recv_sem.at[0])

    def climb(s, level):
        new = jnp.maximum(all_scalars[s, 2:4, :] + level, all_scalars[s, 0:2, :])
        return jnp.where(s < me, new, level)

    anchor = lax.fori_loop(0, 64, climb, jnp.zeros((2, 128), jnp.float32))
    landed(all_pieces, recv_sem.at[1])
    head = me // 32

    def scan(s, held):
        state, level = held
        carries[s] = state
        late = all_scalars[s, pl.ds(head, 1), :]
        moved = all_scalars[s, pl.ds(2 + head, 1), :] + level
        new = jnp.maximum(moved, late)
        state = state * jnp.exp(moved - new) + all_pieces[s] * jnp.exp(late - new)
        return (state, new)

    lax.fori_loop(0, 64, scan, (jnp.zeros((8, 128), jnp.float32), jnp.zeros((1, 128), jnp.float32)))
    others(here, lambda d, dev: copy(carries.at[d], carried.at[me], 2, dev).start())
    carried[me] = carries[me]
    landed(carried, recv_sem.at[2])

    span = length // 2

    def finish(start, store):
        rows = pl.ds(pl.multiple_of(start, span), span)
        for h in range(2):
            state = jnp.concatenate(
                [
                    carried[h * 32 + half * 16 : h * 32 + (half + 1) * 16].reshape(QK, 128)
                    for half in range(2)
                ],
                axis=1,
            ).astype(jnp.bfloat16)
            wide = slice(h * V_DIM, (h + 1) * V_DIM)
            from_state = jnp.dot(
                query_ref[rows, h * QK : (h + 1) * QK], state, preferred_element_type=jnp.float32
            )
            log_inter = columns[rows, h : h + 1] + anchor[h : h + 1, 0:1]
            level = local_level[h, rows, 0:1]
            peak = jnp.maximum(log_inter, level)
            number = (
                jnp.exp(log_inter - peak) * from_state + jnp.exp(level - peak) * local_num[rows, wide]
            )
            scaled = number * lax.rsqrt(
                jnp.mean(number * number, axis=1, keepdims=True) + epsilon
            )
            gate = jax.nn.sigmoid(out_gate_ref[rows, wide].astype(jnp.float32))
            store(h, (scaled * gate).astype(jnp.bfloat16))

    def to_partner(h, value):
        outbox[:, h * V_DIM : (h + 1) * V_DIM] = value

    def to_self(h, value):
        start = pl.multiple_of(core * 2 * V_DIM + h * V_DIM, V_DIM)
        heads[:, pl.ds(start, V_DIM)] = value

    loads["out_gate"].wait()
    finish((1 - core) * span, to_partner)
    mine = pl.ds(pl.multiple_of(core * 2 * V_DIM, 2 * V_DIM), 2 * V_DIM)
    swap = copy(outbox, heads.at[:, mine], 3, partner)
    swap.start()
    weights = [
        pltpu.make_async_remote_copy(
            src_ref=mine_,
            dst_ref=theirs,
            send_sem=weight_send.at[i],
            recv_sem=weight_recv.at[i],
            device_id=partner,
            device_id_type=MESH,
        )
        for i, (mine_, theirs) in enumerate(
            (
                (gate_ref, gate_full.at[:, pl.ds(units, units)]),
                (up_ref, up_full.at[:, pl.ds(units, units)]),
                (down_ref, down_full.at[pl.ds(units, units)]),
            )
        )
    ]
    for weight in weights:
        weight.start()
    finish(core * span, to_self)
    swap.wait()
    loads["out_proj"].wait()
    loads["stream"].wait()
    loads["gain"].wait()
    width = stream_ref.shape[1]
    tiles = [slice(n, n + TILE) for n in range(0, width, TILE)]
    squares = jnp.zeros((stream_ref.shape[0], 1), F32)
    for cols in tiles:
        mix = jnp.dot(heads[...], out_proj_ref[:, cols], preferred_element_type=F32)
        both = (stream_ref[:, cols].astype(F32) + mix).astype(BF16)
        middle_ref[:, cols] = both
        both = both.astype(F32)
        squares = squares + jnp.sum(both * both, axis=1, keepdims=True)
    factor = lax.rsqrt(squares / width + epsilon)
    for cols in tiles:
        normed_ref[:, cols] = (middle_ref[:, cols].astype(F32) * factor * gain_ref[:, cols]).astype(BF16)

    def rows(i):
        return pl.ds(i * SLOT, SLOT)

    def group(g):
        return pl.ds(g * GROUP_ROWS, GROUP_ROWS)

    def members(g):
        return range(max(g * PER_GROUP, 1), (g + 1) * PER_GROUP)

    def build(g):
        pick = select_ref[group(g), :]
        for cols in tiles:
            outgoing[group(g), cols] = jnp.dot(
                pick, normed_ref[:, cols], preferred_element_type=F32
            ).astype(BF16)

    def send(g):
        for i in members(g):
            pltpu.make_async_remote_copy(
                src_ref=outgoing.at[rows(i)],
                dst_ref=arrived.at[rows(i)],
                send_sem=rows_send,
                recv_sem=rows_recv.at[g],
                device_id=peer(here, OFFSETS[i]),
                device_id_type=MESH,
            ).start()

    build(0)
    for g in range(1, GROUPS):
        send(g - 1)
        build(g)
    arrived[rows(0), :] = outgoing[rows(0), :]
    send(GROUPS - 1)

    def all_in(ref, sem, first, last):
        span = ref.at[pl.ds(first * SLOT, (last - first) * SLOT)]
        pltpu.make_async_copy(span, span, sem).wait()

    for name in ("gate", "up", "down"):
        loads[name].wait()
    for weight in weights:
        weight.wait_recv()
    for g in range(GROUPS):
        all_in(arrived, rows_recv.at[g], members(g)[0], members(g)[-1] + 1)
        block = arrived[group(g), :]
        for n in range(0, hidden.shape[1], TILE):
            cols = slice(n, n + TILE)
            gates = jnp.dot(block, gate_full[:, cols], preferred_element_type=F32)
            ups = jnp.dot(block, up_full[:, cols], preferred_element_type=F32)
            hidden[:, cols] = (gates * jax.nn.sigmoid(gates) * ups).astype(BF16)
        for cols in tiles:
            answers[group(g), cols] = jnp.dot(
                hidden[...], down_full[:, cols], preferred_element_type=F32
            ).astype(BF16)
        for i in members(g):
            pltpu.make_async_remote_copy(
                src_ref=answers.at[rows(i)],
                dst_ref=returned.at[rows(i)],
                send_sem=back_send,
                recv_sem=back_recv.at[g],
                device_id=peer(here, OFFSETS[i], -1),
                device_id_type=MESH,
            ).start()
    returned[rows(0), :] = answers[rows(0), :]
    for g in range(GROUPS):
        all_in(returned, back_recv.at[g], members(g)[0], members(g)[-1] + 1)
        for cols in tiles:
            part = jnp.dot(
                weigh_ref[0, :, group(g)], returned[group(g), cols], preferred_element_type=F32
            ) + jnp.dot(
                weigh_ref[1, :, group(g)], returned[group(g), cols], preferred_element_type=F32
            )
            before = middle_ref[:, cols].astype(F32) if g == 0 else total[:, cols]
            if g < GROUPS - 1:
                total[:, cols] = before + part
            else:
                out_ref[:, cols] = (before + part).astype(out_ref.dtype)
    all_in(outgoing, rows_send, 1, len(OFFSETS))
    all_in(answers, back_send, 1, len(OFFSETS))
    for weight in weights:
        weight.wait_send()
    for ref, lane in ((all_scalars, 0), (all_pieces, 1), (carried, 2)):
        landed(ref, send_sem.at[lane])


def body(*arrays):
    (
        stream,
        queries,
        key_rows,
        value_rows,
        out_gate,
        in_gate,
        forget_gate,
        out_proj,
        ffn_gain,
        gate_proj,
        up_proj,
        down_proj,
        expert_ids,
        route_weights,
    ) = arrays
    rows_here, width = stream.shape
    length = queries.shape[0]
    half = gate_proj.shape[2]
    slots = len(OFFSETS) * SLOT
    gain = ffn_gain.reshape(1, width)
    ids, routes = expert_ids.T, route_weights.T
    loaded = [
        stream,
        queries,
        key_rows,
        value_rows,
        out_gate,
        in_gate,
        forget_gate,
        out_proj,
        gain,
        ids,
        routes,
    ]
    vmem, dma = pltpu.VMEM, pltpu.SemaphoreType.DMA
    return pl.pallas_call(
        layer_kernel,
        out_shape=jax.ShapeDtypeStruct((rows_here, width), BF16),
        in_specs=[pl.BlockSpec(memory_space=pl.ANY)] * 14,
        out_specs=pl.BlockSpec(memory_space=pltpu.VMEM),
        scratch_shapes=[vmem(a.shape, a.dtype) for a in loaded]
        + [
            vmem((128, length), F32),
            vmem((length, 128), F32),
            vmem((length, 2 * V_DIM), F32),
            vmem((2, length, 128), F32),
            vmem((4, 128), F32),
            vmem((64, 4, 128), F32),
        ]
        + [vmem((64, 8, 128), F32)] * 4
        + [
            vmem((rows_here, 2 * V_DIM), BF16),
            vmem((rows_here, 4 * V_DIM), BF16),
            vmem((len(OFFSETS), rows_here), F32),
            vmem((len(OFFSETS), rows_here), F32),
            vmem((slots, rows_here), BF16),
            vmem((2, rows_here, slots), BF16),
            vmem((rows_here, width), BF16),
            vmem((rows_here, width), BF16),
        ]
        + [vmem((slots, width), BF16)] * 4
        + [
            vmem((width, 2 * half), BF16),
            vmem((width, 2 * half), BF16),
            vmem((2 * half, width), BF16),
            vmem((GROUP_ROWS, 2 * half), BF16),
            vmem((rows_here, width), F32),
            dma((14,)),
            dma((4,)),
            dma((4,)),
            dma((3,)),
            dma((3,)),
            dma(()),
            dma((GROUPS,)),
            dma(()),
            dma((GROUPS,)),
        ],
        compiler_params=pltpu.CompilerParams(
            collective_id=0, has_side_effects=True, vmem_limit_bytes=62 << 20
        ),
    )(
        stream,
        queries,
        key_rows,
        value_rows,
        out_gate,
        in_gate,
        forget_gate,
        out_proj,
        gain,
        gate_proj[0],
        up_proj[0],
        down_proj[0],
        ids,
        routes,
    )


def solution(mesh):
    split = Mesh(mesh.devices.reshape(4, 4, 4, mesh.shape["tp"]), ("sp_0", "sp_1", "sp_2", "tp"))
    return jax.shard_map(
        body,
        mesh=split,
        in_specs=(
            P(SP_TP, None),
            P(SP, "tp"),
            P(SP, "tp"),
            P(SP, "tp"),
            P(SP, "tp"),
            P("tp", SP),
            P("tp", SP),
            P(),
            P(),
            P(SP, None, "tp"),
            P(SP, None, "tp"),
            P(SP, "tp", None),
            P(SP_TP, None),
            P(SP_TP, None),
        ),
        out_specs=P(SP_TP, None),
        check_vma=False,
    )
```

```python
import jax
import jax.numpy as jnp
from jax import lax
from jax.experimental import pallas as pl
from jax.experimental.pallas import tpu as pltpu
from jax.sharding import Mesh
from jax.sharding import PartitionSpec as P

MESH = pl.DeviceIdType.MESH
QK = 128
V_DIM = 256
SP = ("sp_0", "sp_1", "sp_2")
SP_TP = ("sp_0", "sp_1", "sp_2", "tp")
SLOT = 16
GROUP_ROWS = 256
PER_GROUP = GROUP_ROWS // SLOT
TILE = 256
epsilon = 1e-06
F32 = jnp.float32
BF16 = jnp.bfloat16


def offsets_by_orbit():
    cube = [(a, b, c) for a in range(4) for b in range(4) for c in range(4)]
    seen, orbits = {(0, 0, 0)}, []
    for o in sorted(cube, key=lambda o: sum(min(v, 4 - v) for v in o)):
        orbit = []
        for turn in range(3):
            turned = o[turn:] + o[:turn]
            for p in (turned, tuple(-v % 4 for v in turned)):
                if p not in seen:
                    seen.add(p)
                    orbit.append(p)
        if orbit:
            orbits.append(orbit)
    order = [(0, 0, 0)]
    for orbit in orbits:
        order += orbit
    return order


OFFSETS = offsets_by_orbit()
GROUPS = len(OFFSETS) // PER_GROUP
EARLY_GROUPS = 2
EARLY = EARLY_GROUPS * PER_GROUP
FIRST_WINDOW = 1


def place():
    return [lax.axis_index(axis) for axis in SP_TP]


def peer(here, offset, sign=1):
    z, y, x, core = here
    return tuple(lax.rem(p + (sign * o) % 4, 4) for p, o in zip((z, y, x), offset)) + (core,)


def index_of(device):
    return (device[0] * 4 + device[1]) * 4 + device[2]


FAR_FIRST = sorted(OFFSETS[1:], key=lambda o: -sum(min(v, 4 - v) for v in o))


def others(here, act):
    for offset in FAR_FIRST:
        device = peer(here, offset)
        act(index_of(device), device)


def route(ids_ref, routes_ref, ranks, shares, select_ref, weigh_ref, here, loads):
    loads["ids"].wait()
    loads["routes"].wait()
    named = ids_ref[...].astype(F32)
    tokens = named.shape[1]
    expert = lax.broadcasted_iota(jnp.int32, (len(OFFSETS), tokens), 0).astype(F32)
    first, second = (named[j : j + 1, :] == expert for j in range(2))
    used = jnp.where(first | second, 1.0, 0.0)
    earlier = lax.broadcasted_iota(jnp.int32, (tokens, tokens), 0)
    later = lax.broadcasted_iota(jnp.int32, (tokens, tokens), 1)
    upper = jnp.where(earlier < later, 1.0, 0.0).astype(BF16)
    rank = jnp.dot(used.astype(BF16), upper, preferred_element_type=F32)
    ranks[...] = jnp.where(first | second, rank, -1.0)
    shares[...] = jnp.where(first, routes_ref[0:1, :], 0.0) + jnp.where(second, routes_ref[1:2, :], 0.0)
    slot = lax.broadcasted_iota(jnp.int32, (SLOT, tokens), 0).astype(F32)
    for g in range(GROUPS):
        weights = []
        for i in range(g * PER_GROUP, (g + 1) * PER_GROUP):
            owner = pl.ds(index_of(peer(here, OFFSETS[i])), 1)
            chosen = ranks[owner, :] == slot
            select_ref[pl.ds(i * SLOT, SLOT), :] = jnp.where(chosen, 1.0, 0.0).astype(BF16)
            weights.append(jnp.where(chosen, shares[owner, :], 0.0))
        weigh = jnp.concatenate(weights, axis=0).T
        high = weigh.astype(BF16)
        cols = slice(g * GROUP_ROWS, (g + 1) * GROUP_ROWS)
        weigh_ref[0, :, cols] = high
        weigh_ref[1, :, cols] = (weigh - high.astype(F32)).astype(BF16)


def layer_kernel(
    stream_hbm,
    query_hbm,
    key_hbm,
    value_hbm,
    out_gate_hbm,
    in_gate_hbm,
    forget_hbm,
    out_proj_hbm,
    gain_hbm,
    gate_ref,
    up_ref,
    down_ref,
    ids_hbm,
    routes_hbm,
    out_ref,
    stream_ref,
    query_ref,
    key_ref,
    value_ref,
    out_gate_ref,
    in_gate_ref,
    forget_ref,
    out_proj_ref,
    gain_ref,
    ids_ref,
    routes_ref,
    table,
    columns,
    local_num,
    local_level,
    scalars,
    all_scalars,
    pieces,
    all_pieces,
    carries,
    carried,
    outbox,
    heads,
    ranks,
    shares,
    select_ref,
    weigh_ref,
    middle_ref,
    normed_ref,
    slots_out,
    slots_in,
    outgoing,
    arrived,
    answers,
    returned,
    gate_full,
    up_full,
    down_full,
    hidden,
    total,
    load_sem,
    send_sem,
    recv_sem,
    weight_send,
    weight_recv,
    rows_send,
    rows_recv,
    early_recv,
    heads_send,
    back_send,
    back_recv,
):
    here = place()
    core = here[3]
    me = index_of(here)
    partner = (here[0], here[1], here[2], 1 - core)
    units = gate_ref.shape[1]
    barrier = pltpu.get_barrier_semaphore()
    others(
        here,
        lambda d, dev: pl.semaphore_signal(barrier, inc=1, device_id=dev, device_id_type=MESH),
    )
    pl.semaphore_signal(barrier, inc=1, device_id=partner, device_id_type=MESH)
    loads = {}
    for name, src, dst in (
        ("forget", forget_hbm, forget_ref),
        ("in", in_gate_hbm, in_gate_ref),
        ("key", key_hbm, key_ref),
        ("value", value_hbm, value_ref),
        ("ids", ids_hbm, ids_ref),
        ("routes", routes_hbm, routes_ref),
        ("stream", stream_hbm, stream_ref),
        ("query", query_hbm, query_ref),
        ("out_gate", out_gate_hbm, out_gate_ref),
        ("out_proj", out_proj_hbm, out_proj_ref),
        ("gain", gain_hbm, gain_ref),
        ("gate", gate_ref, gate_full.at[:, pl.ds(0, units)]),
        ("up", up_ref, up_full.at[:, pl.ds(0, units)]),
        ("down", down_ref, down_full.at[pl.ds(0, units)]),
    ):
        loads[name] = pltpu.make_async_copy(src, dst, load_sem.at[len(loads)])
        loads[name].start()

    length = query_ref.shape[0]
    scale = QK ** (-0.5)
    loads["forget"].wait()
    loads["in"].wait()
    x = forget_ref[...]
    u = jnp.exp(-jnp.abs(x))
    small = u * (1.0 - u * (0.5 - u * (1.0 / 3.0 - u * 0.25)))
    decay = jnp.minimum(x, 0.0) - jnp.where(u < 0.01, small, jnp.log(1.0 + u))
    table[...] = jnp.zeros_like(table)
    table[0:2, :] = decay
    raw = table[0:8, :]
    high = raw.astype(jnp.bfloat16).astype(jnp.float32)
    mid = (raw - high).astype(jnp.bfloat16).astype(jnp.float32)
    low = raw - high - mid
    parts = jnp.concatenate([high, mid, low], axis=0).astype(jnp.bfloat16)
    before = lax.broadcasted_iota(jnp.int32, (length, length), 0)
    after = lax.broadcasted_iota(jnp.int32, (length, length), 1)
    upper = jnp.where(before <= after, 1.0, 0.0).astype(jnp.bfloat16)
    summed = jnp.dot(parts, upper, preferred_element_type=jnp.float32)
    summed = summed[0:8] + summed[8:16] + summed[16:24]
    table[0:2, :] = summed[0:2]
    table[2:4, :] = in_gate_ref[...]
    columns[...] = table[...].T
    rows_a, peaks = [], []
    for h in range(2):
        row_a = table[2 + h : 3 + h, :] - table[h : h + 1, :]
        peak = jnp.max(row_a, axis=1, keepdims=True)
        closing = table[h : h + 1, length - 1 : length]
        scalars[h : h + 1, :] = jnp.broadcast_to(closing + peak, (1, 128))
        scalars[2 + h : 3 + h, :] = jnp.broadcast_to(closing, (1, 128))
        rows_a.append(row_a)
        peaks.append(peak)
    loads["key"].wait()
    loads["value"].wait()
    for h in range(2):
        col_a = columns[:, 2 + h : 3 + h] - columns[:, h : h + 1]
        weight = jnp.exp(col_a - peaks[h]) * scale
        keys = (key_ref[:, h * QK : (h + 1) * QK].astype(jnp.float32) * weight).astype(jnp.bfloat16)
        state = lax.dot_general(
            keys,
            value_ref[:, h * V_DIM : (h + 1) * V_DIM],
            (((0,), (0,)), ((), ())),
            preferred_element_type=jnp.float32,
        )
        for half in range(2):
            at = h * 32 + half * 16
            pieces[at : at + 16] = state[:, half * 128 : (half + 1) * 128].reshape(16, 8, 128)
    route(ids_ref, routes_ref, ranks, shares, select_ref, weigh_ref, here, loads)
    width = stream_ref.shape[1]
    tiles = [slice(n, n + TILE) for n in range(0, width, TILE)]

    def spot(i):
        return pl.ds(i * SLOT, SLOT)

    def group(g):
        return pl.ds(g * GROUP_ROWS, GROUP_ROWS)

    def members(g):
        return range(max(g * PER_GROUP, 1), (g + 1) * PER_GROUP)

    def fill(g, source, target):
        pick = select_ref[group(g), :]
        for n in range(0, source.shape[1], TILE):
            cols = slice(n, n + TILE)
            target[group(g), cols] = jnp.dot(
                pick, source[:, cols], preferred_element_type=F32
            ).astype(BF16)

    def push(source, target, blocks, sends, lands, sign=1):
        for i in blocks:
            pltpu.make_async_remote_copy(
                src_ref=source.at[spot(i)],
                dst_ref=target.at[spot(i)],
                send_sem=sends,
                recv_sem=lands,
                device_id=peer(here, OFFSETS[i], sign),
                device_id_type=MESH,
            ).start()

    def all_in(ref, sem, first, last):
        span = ref.at[pl.ds(first * SLOT, (last - first) * SLOT)]
        pltpu.make_async_copy(span, span, sem).wait()

    loads["stream"].wait()
    for g in range(EARLY_GROUPS):
        fill(g, stream_ref, outgoing)
    arrived[spot(0), :] = outgoing[spot(0), :]
    pl.semaphore_wait(barrier, 64)

    def copy(src, dst, lane, dev):
        return pltpu.make_async_remote_copy(
            src_ref=src,
            dst_ref=dst,
            send_sem=send_sem.at[lane],
            recv_sem=recv_sem.at[lane],
            device_id=dev,
            device_id_type=MESH,
        )

    def landed(ref, sem):
        span = ref.at[pl.ds(0, 63)]
        pltpu.make_async_copy(span, span, sem).wait()

    def spread(d, dev):
        copy(scalars, all_scalars.at[me], 0, dev).start()
        copy(pieces.at[d], all_pieces.at[me], 1, dev).start()

    others(here, spread)
    for g in range(EARLY_GROUPS):
        push(outgoing, arrived, [i for i in members(g) if i < FIRST_WINDOW], rows_send, early_recv.at[g])
    all_scalars[me] = scalars[...]
    all_pieces[me] = pieces[me]

    loads["query"].wait()
    step = 128
    for h in range(2):
        for r in range(length // step):
            n = (r + 1) * step
            rows = slice(r * step, n)
            score = lax.dot_general(
                query_ref[rows, h * QK : (h + 1) * QK],
                key_ref[0:n, h * QK : (h + 1) * QK],
                (((1,), (1,)), ((), ())),
                preferred_element_type=jnp.float32,
            )
            t = lax.broadcasted_iota(jnp.int32, (step, n), 0) + r * step
            s = lax.broadcasted_iota(jnp.int32, (step, n), 1)
            log_inner = jnp.where(s <= t, columns[rows, h : h + 1] + rows_a[h][:, 0:n], -1e30)
            level = jnp.max(log_inner, axis=1, keepdims=True)
            score = (score * scale * jnp.exp(log_inner - level)).astype(jnp.bfloat16)
            local_num[rows, h * V_DIM : (h + 1) * V_DIM] = jnp.dot(
                score, value_ref[0:n, h * V_DIM : (h + 1) * V_DIM], preferred_element_type=jnp.float32
            )
            local_level[h, rows, :] = jnp.broadcast_to(level, (step, 128))

    landed(all_scalars, recv_sem.at[0])

    def climb(s, level):
        new = jnp.maximum(all_scalars[s, 2:4, :] + level, all_scalars[s, 0:2, :])
        return jnp.where(s < me, new, level)

    anchor = lax.fori_loop(0, 64, climb, jnp.zeros((2, 128), jnp.float32))
    landed(all_pieces, recv_sem.at[1])
    head = me // 32

    def scan(s, held):
        state, level = held
        carries[s] = state
        late = all_scalars[s, pl.ds(head, 1), :]
        moved = all_scalars[s, pl.ds(2 + head, 1), :] + level
        new = jnp.maximum(moved, late)
        state = state * jnp.exp(moved - new) + all_pieces[s] * jnp.exp(late - new)
        return (state, new)

    lax.fori_loop(0, 64, scan, (jnp.zeros((8, 128), jnp.float32), jnp.zeros((1, 128), jnp.float32)))
    others(here, lambda d, dev: copy(carries.at[d], carried.at[me], 2, dev).start())
    weights = [
        pltpu.make_async_remote_copy(
            src_ref=mine_,
            dst_ref=theirs,
            send_sem=weight_send.at[i],
            recv_sem=weight_recv.at[i],
            device_id=partner,
            device_id_type=MESH,
        )
        for i, (mine_, theirs) in enumerate(
            (
                (gate_ref, gate_full.at[:, pl.ds(units, units)]),
                (up_ref, up_full.at[:, pl.ds(units, units)]),
                (down_ref, down_full.at[pl.ds(units, units)]),
            )
        )
    ]
    for weight in weights:
        weight.start()
    for g in range(EARLY_GROUPS):
        push(outgoing, arrived, [i for i in members(g) if i >= FIRST_WINDOW], rows_send, early_recv.at[g])
    carried[me] = carries[me]
    landed(carried, recv_sem.at[2])

    span = length // 2

    def finish(start, store):
        rows = pl.ds(pl.multiple_of(start, span), span)
        for h in range(2):
            state = jnp.concatenate(
                [
                    carried[h * 32 + half * 16 : h * 32 + (half + 1) * 16].reshape(QK, 128)
                    for half in range(2)
                ],
                axis=1,
            ).astype(jnp.bfloat16)
            wide = slice(h * V_DIM, (h + 1) * V_DIM)
            from_state = jnp.dot(
                query_ref[rows, h * QK : (h + 1) * QK], state, preferred_element_type=jnp.float32
            )
            log_inter = columns[rows, h : h + 1] + anchor[h : h + 1, 0:1]
            level = local_level[h, rows, 0:1]
            peak = jnp.maximum(log_inter, level)
            number = (
                jnp.exp(log_inter - peak) * from_state + jnp.exp(level - peak) * local_num[rows, wide]
            )
            scaled = number * lax.rsqrt(
                jnp.mean(number * number, axis=1, keepdims=True) + epsilon
            )
            gate = jax.nn.sigmoid(out_gate_ref[rows, wide].astype(jnp.float32))
            store(h, (scaled * gate).astype(jnp.bfloat16))

    def to_partner(h, value):
        outbox[:, h * V_DIM : (h + 1) * V_DIM] = value

    def to_self(h, value):
        start = pl.multiple_of(core * 2 * V_DIM + h * V_DIM, V_DIM)
        heads[:, pl.ds(start, V_DIM)] = value

    loads["out_gate"].wait()
    finish((1 - core) * span, to_partner)
    mine = pl.ds(pl.multiple_of(core * 2 * V_DIM, 2 * V_DIM), 2 * V_DIM)
    swap = copy(outbox, heads.at[:, mine], 3, partner)
    swap.start()
    finish(core * span, to_self)
    swap.wait()
    for g in range(EARLY_GROUPS):
        fill(g, heads, slots_out)
        push(slots_out, slots_in, members(g), heads_send, rows_recv.at[g])
    slots_in[spot(0), :] = slots_out[spot(0), :]
    loads["out_proj"].wait()
    loads["gain"].wait()
    squares = jnp.zeros((stream_ref.shape[0], 1), F32)
    for cols in tiles:
        mix = jnp.dot(heads[...], out_proj_ref[:, cols], preferred_element_type=F32)
        both = (stream_ref[:, cols].astype(F32) + mix).astype(BF16)
        middle_ref[:, cols] = both
        both = both.astype(F32)
        squares = squares + jnp.sum(both * both, axis=1, keepdims=True)
    factor = lax.rsqrt(squares / width + epsilon)
    for cols in tiles:
        normed_ref[:, cols] = (middle_ref[:, cols].astype(F32) * factor * gain_ref[:, cols]).astype(BF16)

    for g in range(EARLY_GROUPS, GROUPS):
        fill(g, normed_ref, outgoing)
        push(outgoing, arrived, members(g), rows_send, rows_recv.at[g])

    for name in ("gate", "up", "down"):
        loads[name].wait()
    for weight in weights:
        weight.wait_recv()
    for g in range(GROUPS):
        if g < EARLY_GROUPS:
            first = members(g)[0]
            all_in(arrived, early_recv.at[g], first, (g + 1) * PER_GROUP)
            all_in(slots_in, rows_recv.at[g], first, (g + 1) * PER_GROUP)
            squares = jnp.zeros((GROUP_ROWS, 1), F32)
            for cols in tiles:
                mix = jnp.dot(slots_in[group(g), :], out_proj_ref[:, cols], preferred_element_type=F32)
                both = (arrived[group(g), cols].astype(F32) + mix).astype(BF16)
                arrived[group(g), cols] = both
                both = both.astype(F32)
                squares = squares + jnp.sum(both * both, axis=1, keepdims=True)
            factor = lax.rsqrt(squares / width + epsilon)
            for cols in tiles:
                arrived[group(g), cols] = (
                    arrived[group(g), cols].astype(F32) * factor * gain_ref[:, cols]
                ).astype(BF16)
        else:
            all_in(arrived, rows_recv.at[g], members(g)[0], members(g)[-1] + 1)
        block = arrived[group(g), :]
        for n in range(0, hidden.shape[1], TILE):
            cols = slice(n, n + TILE)
            gates = jnp.dot(block, gate_full[:, cols], preferred_element_type=F32)
            ups = jnp.dot(block, up_full[:, cols], preferred_element_type=F32)
            hidden[:, cols] = (gates * jax.nn.sigmoid(gates) * ups).astype(BF16)
        for cols in tiles:
            answers[group(g), cols] = jnp.dot(
                hidden[...], down_full[:, cols], preferred_element_type=F32
            ).astype(BF16)
        push(answers, returned, members(g), back_send, back_recv.at[g], -1)
    returned[spot(0), :] = answers[spot(0), :]
    for g in range(GROUPS):
        all_in(returned, back_recv.at[g], members(g)[0], members(g)[-1] + 1)
        for cols in tiles:
            part = jnp.dot(
                weigh_ref[0, :, group(g)], returned[group(g), cols], preferred_element_type=F32
            ) + jnp.dot(
                weigh_ref[1, :, group(g)], returned[group(g), cols], preferred_element_type=F32
            )
            before = middle_ref[:, cols].astype(F32) if g == 0 else total[:, cols]
            if g < GROUPS - 1:
                total[:, cols] = before + part
            else:
                out_ref[:, cols] = (before + part).astype(out_ref.dtype)
    all_in(outgoing, rows_send, 1, len(OFFSETS))
    all_in(answers, back_send, 1, len(OFFSETS))
    all_in(slots_out, heads_send, 1, EARLY)
    for weight in weights:
        weight.wait_send()
    for ref, lane in ((all_scalars, 0), (all_pieces, 1), (carried, 2)):
        landed(ref, send_sem.at[lane])


def body(*arrays):
    (
        stream,
        queries,
        key_rows,
        value_rows,
        out_gate,
        in_gate,
        forget_gate,
        out_proj,
        ffn_gain,
        gate_proj,
        up_proj,
        down_proj,
        expert_ids,
        route_weights,
    ) = arrays
    rows_here, width = stream.shape
    length = queries.shape[0]
    half = gate_proj.shape[2]
    slots = len(OFFSETS) * SLOT
    gain = ffn_gain.reshape(1, width)
    ids, routes = expert_ids.T, route_weights.T
    loaded = [
        stream,
        queries,
        key_rows,
        value_rows,
        out_gate,
        in_gate,
        forget_gate,
        out_proj,
        gain,
        ids,
        routes,
    ]
    vmem, dma = pltpu.VMEM, pltpu.SemaphoreType.DMA
    return pl.pallas_call(
        layer_kernel,
        out_shape=jax.ShapeDtypeStruct((rows_here, width), BF16),
        in_specs=[pl.BlockSpec(memory_space=pl.ANY)] * 14,
        out_specs=pl.BlockSpec(memory_space=pltpu.VMEM),
        scratch_shapes=[vmem(a.shape, a.dtype) for a in loaded]
        + [
            vmem((128, length), F32),
            vmem((length, 128), F32),
            vmem((length, 2 * V_DIM), F32),
            vmem((2, length, 128), F32),
            vmem((4, 128), F32),
            vmem((64, 4, 128), F32),
        ]
        + [vmem((64, 8, 128), F32)] * 4
        + [
            vmem((rows_here, 2 * V_DIM), BF16),
            vmem((rows_here, 4 * V_DIM), BF16),
            vmem((len(OFFSETS), rows_here), F32),
            vmem((len(OFFSETS), rows_here), F32),
            vmem((slots, rows_here), BF16),
            vmem((2, rows_here, slots), BF16),
            vmem((rows_here, width), BF16),
            vmem((rows_here, width), BF16),
        ]
        + [vmem((EARLY * SLOT, 4 * V_DIM), BF16)] * 2
        + [vmem((slots, width), BF16)] * 4
        + [
            vmem((width, 2 * half), BF16),
            vmem((width, 2 * half), BF16),
            vmem((2 * half, width), BF16),
            vmem((GROUP_ROWS, 2 * half), BF16),
            vmem((rows_here, width), F32),
            dma((14,)),
            dma((4,)),
            dma((4,)),
            dma((3,)),
            dma((3,)),
            dma(()),
            dma((GROUPS,)),
            dma((EARLY_GROUPS,)),
            dma(()),
            dma(()),
            dma((GROUPS,)),
        ],
        compiler_params=pltpu.CompilerParams(
            collective_id=0, has_side_effects=True, vmem_limit_bytes=62 << 20
        ),
    )(
        stream,
        queries,
        key_rows,
        value_rows,
        out_gate,
        in_gate,
        forget_gate,
        out_proj,
        gain,
        gate_proj[0],
        up_proj[0],
        down_proj[0],
        ids,
        routes,
    )


def solution(mesh):
    split = Mesh(mesh.devices.reshape(4, 4, 4, mesh.shape["tp"]), ("sp_0", "sp_1", "sp_2", "tp"))
    return jax.shard_map(
        body,
        mesh=split,
        in_specs=(
            P(SP_TP, None),
            P(SP, "tp"),
            P(SP, "tp"),
            P(SP, "tp"),
            P(SP, "tp"),
            P("tp", SP),
            P("tp", SP),
            P(),
            P(),
            P(SP, None, "tp"),
            P(SP, None, "tp"),
            P(SP, "tp", None),
            P(SP_TP, None),
            P(SP_TP, None),
        ),
        out_specs=P(SP_TP, None),
        check_vma=False,
    )
```

```python
import jax
import jax.numpy as jnp
from jax import lax
from jax.experimental import pallas as pl
from jax.experimental.pallas import tpu as pltpu
from jax.sharding import Mesh
from jax.sharding import PartitionSpec as P

MESH = pl.DeviceIdType.MESH
QK = 128
V_DIM = 256
SP = ("sp_0", "sp_1", "sp_2")
SP_TP = ("sp_0", "sp_1", "sp_2", "tp")
SLOT = 16
GROUP_ROWS = 256
PER_GROUP = GROUP_ROWS // SLOT
TILE = 256
epsilon = 1e-06
F32 = jnp.float32
BF16 = jnp.bfloat16


def offsets_by_orbit():
    cube = [(a, b, c) for a in range(4) for b in range(4) for c in range(4)]
    seen, orbits = {(0, 0, 0)}, []
    for o in sorted(cube, key=lambda o: sum(min(v, 4 - v) for v in o)):
        orbit = []
        for turn in range(3):
            turned = o[turn:] + o[:turn]
            for p in (turned, tuple(-v % 4 for v in turned)):
                if p not in seen:
                    seen.add(p)
                    orbit.append(p)
        if orbit:
            orbits.append(orbit)
    order = [(0, 0, 0)]
    for orbit in orbits:
        order += orbit
    return order


OFFSETS = offsets_by_orbit()
GROUPS = len(OFFSETS) // PER_GROUP
EARLY_GROUPS = 2
EARLY = EARLY_GROUPS * PER_GROUP
FIRST_WINDOW = 7


def place():
    return [lax.axis_index(axis) for axis in SP_TP]


def peer(here, offset, sign=1):
    z, y, x, core = here
    return tuple(lax.rem(p + (sign * o) % 4, 4) for p, o in zip((z, y, x), offset)) + (core,)


def index_of(device):
    return (device[0] * 4 + device[1]) * 4 + device[2]


FAR_FIRST = sorted(OFFSETS[1:], key=lambda o: -sum(min(v, 4 - v) for v in o))


def others(here, act):
    for offset in FAR_FIRST:
        device = peer(here, offset)
        act(index_of(device), device)


def route(ids_ref, routes_ref, ranks, shares, select_ref, weigh_ref, here, loads):
    loads["ids"].wait()
    loads["routes"].wait()
    named = ids_ref[...].astype(F32)
    tokens = named.shape[1]
    expert = lax.broadcasted_iota(jnp.int32, (len(OFFSETS), tokens), 0).astype(F32)
    first, second = (named[j : j + 1, :] == expert for j in range(2))
    used = jnp.where(first | second, 1.0, 0.0)
    earlier = lax.broadcasted_iota(jnp.int32, (tokens, tokens), 0)
    later = lax.broadcasted_iota(jnp.int32, (tokens, tokens), 1)
    upper = jnp.where(earlier < later, 1.0, 0.0).astype(BF16)
    rank = jnp.dot(used.astype(BF16), upper, preferred_element_type=F32)
    ranks[...] = jnp.where(first | second, rank, -1.0)
    shares[...] = jnp.where(first, routes_ref[0:1, :], 0.0) + jnp.where(second, routes_ref[1:2, :], 0.0)
    slot = lax.broadcasted_iota(jnp.int32, (SLOT, tokens), 0).astype(F32)
    for g in range(GROUPS):
        weights = []
        for i in range(g * PER_GROUP, (g + 1) * PER_GROUP):
            owner = pl.ds(index_of(peer(here, OFFSETS[i])), 1)
            chosen = ranks[owner, :] == slot
            select_ref[pl.ds(i * SLOT, SLOT), :] = jnp.where(chosen, 1.0, 0.0).astype(BF16)
            weights.append(jnp.where(chosen, shares[owner, :], 0.0))
        weigh = jnp.concatenate(weights, axis=0).T
        high = weigh.astype(BF16)
        cols = slice(g * GROUP_ROWS, (g + 1) * GROUP_ROWS)
        weigh_ref[0, :, cols] = high
        weigh_ref[1, :, cols] = (weigh - high.astype(F32)).astype(BF16)


def layer_kernel(
    stream_hbm,
    query_hbm,
    key_hbm,
    value_hbm,
    out_gate_hbm,
    in_gate_hbm,
    forget_hbm,
    out_proj_hbm,
    gain_hbm,
    gate_ref,
    up_ref,
    down_ref,
    ids_hbm,
    routes_hbm,
    out_ref,
    stream_ref,
    query_ref,
    key_ref,
    value_ref,
    out_gate_ref,
    in_gate_ref,
    forget_ref,
    out_proj_ref,
    gain_ref,
    ids_ref,
    routes_ref,
    table,
    columns,
    local_num,
    local_level,
    gates_ref,
    scalars,
    all_scalars,
    pieces,
    all_pieces,
    carries,
    carried,
    outbox,
    heads,
    ranks,
    shares,
    select_ref,
    weigh_ref,
    middle_ref,
    normed_ref,
    slots_out,
    slots_in,
    outgoing,
    arrived,
    answers,
    returned,
    gate_full,
    up_full,
    down_full,
    hidden,
    total,
    load_sem,
    send_sem,
    recv_sem,
    weight_send,
    weight_recv,
    rows_send,
    rows_recv,
    early_recv,
    heads_send,
    back_send,
    back_recv,
):
    here = place()
    core = here[3]
    me = index_of(here)
    partner = (here[0], here[1], here[2], 1 - core)
    units = gate_ref.shape[1]
    barrier = pltpu.get_barrier_semaphore()
    others(
        here,
        lambda d, dev: pl.semaphore_signal(barrier, inc=1, device_id=dev, device_id_type=MESH),
    )
    pl.semaphore_signal(barrier, inc=1, device_id=partner, device_id_type=MESH)
    loads = {}
    for name, src, dst in (
        ("forget", forget_hbm, forget_ref),
        ("in", in_gate_hbm, in_gate_ref),
        ("key", key_hbm, key_ref),
        ("value", value_hbm, value_ref),
        ("ids", ids_hbm, ids_ref),
        ("routes", routes_hbm, routes_ref),
        ("stream", stream_hbm, stream_ref),
        ("query", query_hbm, query_ref),
        ("out_gate", out_gate_hbm, out_gate_ref),
        ("out_proj", out_proj_hbm, out_proj_ref),
        ("gain", gain_hbm, gain_ref),
        ("gate", gate_ref, gate_full.at[:, pl.ds(0, units)]),
        ("up", up_ref, up_full.at[:, pl.ds(0, units)]),
        ("down", down_ref, down_full.at[pl.ds(0, units)]),
    ):
        loads[name] = pltpu.make_async_copy(src, dst, load_sem.at[len(loads)])
        loads[name].start()

    length = query_ref.shape[0]
    scale = QK ** (-0.5)
    loads["forget"].wait()
    loads["in"].wait()
    x = forget_ref[...]
    u = jnp.exp(-jnp.abs(x))
    small = u * (1.0 - u * (0.5 - u * (1.0 / 3.0 - u * 0.25)))
    decay = jnp.minimum(x, 0.0) - jnp.where(u < 0.01, small, jnp.log(1.0 + u))
    table[...] = jnp.zeros_like(table)
    table[0:2, :] = decay
    raw = table[0:8, :]
    high = raw.astype(jnp.bfloat16).astype(jnp.float32)
    mid = (raw - high).astype(jnp.bfloat16).astype(jnp.float32)
    low = raw - high - mid
    parts = jnp.concatenate([high, mid, low], axis=0).astype(jnp.bfloat16)
    before = lax.broadcasted_iota(jnp.int32, (length, length), 0)
    after = lax.broadcasted_iota(jnp.int32, (length, length), 1)
    upper = jnp.where(before <= after, 1.0, 0.0).astype(jnp.bfloat16)
    summed = jnp.dot(parts, upper, preferred_element_type=jnp.float32)
    summed = summed[0:8] + summed[8:16] + summed[16:24]
    table[0:2, :] = summed[0:2]
    table[2:4, :] = in_gate_ref[...]
    columns[...] = table[...].T
    rows_a, peaks = [], []
    for h in range(2):
        row_a = table[2 + h : 3 + h, :] - table[h : h + 1, :]
        peak = jnp.max(row_a, axis=1, keepdims=True)
        closing = table[h : h + 1, length - 1 : length]
        scalars[h : h + 1, :] = jnp.broadcast_to(closing + peak, (1, 128))
        scalars[2 + h : 3 + h, :] = jnp.broadcast_to(closing, (1, 128))
        rows_a.append(row_a)
        peaks.append(peak)
    loads["key"].wait()
    loads["value"].wait()
    for h in range(2):
        col_a = columns[:, 2 + h : 3 + h] - columns[:, h : h + 1]
        weight = jnp.exp(col_a - peaks[h]) * scale
        keys = (key_ref[:, h * QK : (h + 1) * QK].astype(jnp.float32) * weight).astype(jnp.bfloat16)
        state = lax.dot_general(
            keys,
            value_ref[:, h * V_DIM : (h + 1) * V_DIM],
            (((0,), (0,)), ((), ())),
            preferred_element_type=jnp.float32,
        )
        for half in range(2):
            at = h * 32 + half * 16
            pieces[at : at + 16] = state[:, half * 128 : (half + 1) * 128].reshape(16, 8, 128)
    route(ids_ref, routes_ref, ranks, shares, select_ref, weigh_ref, here, loads)
    width = stream_ref.shape[1]
    tiles = [slice(n, n + TILE) for n in range(0, width, TILE)]

    def spot(i):
        return pl.ds(i * SLOT, SLOT)

    def group(g):
        return pl.ds(g * GROUP_ROWS, GROUP_ROWS)

    def members(g):
        return range(max(g * PER_GROUP, 1), (g + 1) * PER_GROUP)

    def fill(g, source, target):
        pick = select_ref[group(g), :]
        for n in range(0, source.shape[1], TILE):
            cols = slice(n, n + TILE)
            target[group(g), cols] = jnp.dot(
                pick, source[:, cols], preferred_element_type=F32
            ).astype(BF16)

    def push(source, target, blocks, sends, lands, sign=1):
        for i in blocks:
            pltpu.make_async_remote_copy(
                src_ref=source.at[spot(i)],
                dst_ref=target.at[spot(i)],
                send_sem=sends,
                recv_sem=lands,
                device_id=peer(here, OFFSETS[i], sign),
                device_id_type=MESH,
            ).start()

    def all_in(ref, sem, first, last):
        span = ref.at[pl.ds(first * SLOT, (last - first) * SLOT)]
        pltpu.make_async_copy(span, span, sem).wait()

    loads["stream"].wait()
    for g in range(EARLY_GROUPS):
        fill(g, stream_ref, outgoing)
    arrived[spot(0), :] = outgoing[spot(0), :]
    pl.semaphore_wait(barrier, 64)

    def copy(src, dst, lane, dev):
        return pltpu.make_async_remote_copy(
            src_ref=src,
            dst_ref=dst,
            send_sem=send_sem.at[lane],
            recv_sem=recv_sem.at[lane],
            device_id=dev,
            device_id_type=MESH,
        )

    def landed(ref, sem):
        span = ref.at[pl.ds(0, 63)]
        pltpu.make_async_copy(span, span, sem).wait()

    def spread(d, dev):
        copy(scalars, all_scalars.at[me], 0, dev).start()
        copy(pieces.at[d], all_pieces.at[me], 1, dev).start()

    others(here, spread)
    for g in range(EARLY_GROUPS):
        push(outgoing, arrived, [i for i in members(g) if i < FIRST_WINDOW], rows_send, early_recv.at[g])
    all_scalars[me] = scalars[...]
    all_pieces[me] = pieces[me]

    loads["query"].wait()
    step = 128
    for h in range(2):
        for r in range(length // step):
            n = (r + 1) * step
            rows = slice(r * step, n)
            score = lax.dot_general(
                query_ref[rows, h * QK : (h + 1) * QK],
                key_ref[0:n, h * QK : (h + 1) * QK],
                (((1,), (1,)), ((), ())),
                preferred_element_type=jnp.float32,
            )
            t = lax.broadcasted_iota(jnp.int32, (step, n), 0) + r * step
            s = lax.broadcasted_iota(jnp.int32, (step, n), 1)
            log_inner = jnp.where(s <= t, columns[rows, h : h + 1] + rows_a[h][:, 0:n], -1e30)
            level = jnp.max(log_inner, axis=1, keepdims=True)
            score = (score * scale * jnp.exp(log_inner - level)).astype(jnp.bfloat16)
            local_num[rows, h * V_DIM : (h + 1) * V_DIM] = jnp.dot(
                score, value_ref[0:n, h * V_DIM : (h + 1) * V_DIM], preferred_element_type=jnp.float32
            )
            local_level[h, rows, :] = jnp.broadcast_to(level, (step, 128))

    landed(all_scalars, recv_sem.at[0])

    def climb(s, level):
        new = jnp.maximum(all_scalars[s, 2:4, :] + level, all_scalars[s, 0:2, :])
        return jnp.where(s < me, new, level)

    anchor = lax.fori_loop(0, 64, climb, jnp.zeros((2, 128), jnp.float32))
    landed(all_pieces, recv_sem.at[1])
    head = me // 32

    def scan(s, held):
        state, level = held
        carries[s] = state
        late = all_scalars[s, pl.ds(head, 1), :]
        moved = all_scalars[s, pl.ds(2 + head, 1), :] + level
        new = jnp.maximum(moved, late)
        state = state * jnp.exp(moved - new) + all_pieces[s] * jnp.exp(late - new)
        return (state, new)

    lax.fori_loop(0, 64, scan, (jnp.zeros((8, 128), jnp.float32), jnp.zeros((1, 128), jnp.float32)))
    others(here, lambda d, dev: copy(carries.at[d], carried.at[me], 2, dev).start())
    weights = [
        pltpu.make_async_remote_copy(
            src_ref=mine_,
            dst_ref=theirs,
            send_sem=weight_send.at[i],
            recv_sem=weight_recv.at[i],
            device_id=partner,
            device_id_type=MESH,
        )
        for i, (mine_, theirs) in enumerate(
            (
                (gate_ref, gate_full.at[:, pl.ds(units, units)]),
                (up_ref, up_full.at[:, pl.ds(units, units)]),
                (down_ref, down_full.at[pl.ds(units, units)]),
            )
        )
    ]
    for weight in weights:
        weight.start()
    for g in range(EARLY_GROUPS):
        push(outgoing, arrived, [i for i in members(g) if i >= FIRST_WINDOW], rows_send, early_recv.at[g])
    carried[me] = carries[me]
    loads["out_gate"].wait()
    for h in range(2):
        wide = slice(h * V_DIM, (h + 1) * V_DIM)
        log_inter = columns[:, h : h + 1] + anchor[h : h + 1, 0:1]
        level = local_level[h, :, 0:1]
        peak = jnp.maximum(log_inter, level)
        local_num[:, wide] = jnp.exp(level - peak) * local_num[:, wide]
        local_level[h] = jnp.broadcast_to(jnp.exp(log_inter - peak), (length, 128))
        gates_ref[:, wide] = jax.nn.sigmoid(out_gate_ref[:, wide].astype(F32))
    landed(carried, recv_sem.at[2])

    span = length // 2

    def finish(start, store):
        rows = pl.ds(pl.multiple_of(start, span), span)
        for h in range(2):
            state = jnp.concatenate(
                [
                    carried[h * 32 + half * 16 : h * 32 + (half + 1) * 16].reshape(QK, 128)
                    for half in range(2)
                ],
                axis=1,
            ).astype(jnp.bfloat16)
            wide = slice(h * V_DIM, (h + 1) * V_DIM)
            from_state = jnp.dot(
                query_ref[rows, h * QK : (h + 1) * QK], state, preferred_element_type=jnp.float32
            )
            number = local_level[h, rows, 0:1] * from_state + local_num[rows, wide]
            scaled = number * lax.rsqrt(
                jnp.mean(number * number, axis=1, keepdims=True) + epsilon
            )
            store(h, (scaled * gates_ref[rows, wide]).astype(jnp.bfloat16))

    def to_partner(h, value):
        outbox[:, h * V_DIM : (h + 1) * V_DIM] = value

    def to_self(h, value):
        start = pl.multiple_of(core * 2 * V_DIM + h * V_DIM, V_DIM)
        heads[:, pl.ds(start, V_DIM)] = value

    finish((1 - core) * span, to_partner)
    mine = pl.ds(pl.multiple_of(core * 2 * V_DIM, 2 * V_DIM), 2 * V_DIM)
    swap = copy(outbox, heads.at[:, mine], 3, partner)
    swap.start()
    finish(core * span, to_self)
    swap.wait()
    for g in range(EARLY_GROUPS):
        fill(g, heads, slots_out)
        push(slots_out, slots_in, members(g), heads_send, rows_recv.at[g])
    slots_in[spot(0), :] = slots_out[spot(0), :]
    loads["out_proj"].wait()
    loads["gain"].wait()
    squares = jnp.zeros((stream_ref.shape[0], 1), F32)
    for cols in tiles:
        mix = jnp.dot(heads[...], out_proj_ref[:, cols], preferred_element_type=F32)
        both = (stream_ref[:, cols].astype(F32) + mix).astype(BF16)
        middle_ref[:, cols] = both
        both = both.astype(F32)
        squares = squares + jnp.sum(both * both, axis=1, keepdims=True)
    factor = lax.rsqrt(squares / width + epsilon)
    for cols in tiles:
        normed_ref[:, cols] = (middle_ref[:, cols].astype(F32) * factor * gain_ref[:, cols]).astype(BF16)

    for g in range(EARLY_GROUPS, GROUPS):
        fill(g, normed_ref, outgoing)
        push(outgoing, arrived, members(g), rows_send, rows_recv.at[g])

    for name in ("gate", "up", "down"):
        loads[name].wait()
    for weight in weights:
        weight.wait_recv()
    for g in range(GROUPS):
        if g < EARLY_GROUPS:
            first = members(g)[0]
            all_in(arrived, early_recv.at[g], first, (g + 1) * PER_GROUP)
            all_in(slots_in, rows_recv.at[g], first, (g + 1) * PER_GROUP)
            squares = jnp.zeros((GROUP_ROWS, 1), F32)
            for cols in tiles:
                mix = jnp.dot(slots_in[group(g), :], out_proj_ref[:, cols], preferred_element_type=F32)
                both = (arrived[group(g), cols].astype(F32) + mix).astype(BF16)
                arrived[group(g), cols] = both
                both = both.astype(F32)
                squares = squares + jnp.sum(both * both, axis=1, keepdims=True)
            factor = lax.rsqrt(squares / width + epsilon)
            for cols in tiles:
                arrived[group(g), cols] = (
                    arrived[group(g), cols].astype(F32) * factor * gain_ref[:, cols]
                ).astype(BF16)
        else:
            all_in(arrived, rows_recv.at[g], members(g)[0], members(g)[-1] + 1)
        block = arrived[group(g), :]
        for n in range(0, hidden.shape[1], TILE):
            cols = slice(n, n + TILE)
            gates = jnp.dot(block, gate_full[:, cols], preferred_element_type=F32)
            ups = jnp.dot(block, up_full[:, cols], preferred_element_type=F32)
            hidden[:, cols] = (gates * jax.nn.sigmoid(gates) * ups).astype(BF16)
        for cols in tiles:
            answers[group(g), cols] = jnp.dot(
                hidden[...], down_full[:, cols], preferred_element_type=F32
            ).astype(BF16)
        push(answers, returned, members(g), back_send, back_recv.at[g], -1)
    returned[spot(0), :] = answers[spot(0), :]
    for g in range(GROUPS):
        all_in(returned, back_recv.at[g], members(g)[0], members(g)[-1] + 1)
        for cols in tiles:
            part = jnp.dot(
                weigh_ref[0, :, group(g)], returned[group(g), cols], preferred_element_type=F32
            ) + jnp.dot(
                weigh_ref[1, :, group(g)], returned[group(g), cols], preferred_element_type=F32
            )
            before = middle_ref[:, cols].astype(F32) if g == 0 else total[:, cols]
            if g < GROUPS - 1:
                total[:, cols] = before + part
            else:
                out_ref[:, cols] = (before + part).astype(out_ref.dtype)
    all_in(outgoing, rows_send, 1, len(OFFSETS))
    all_in(answers, back_send, 1, len(OFFSETS))
    all_in(slots_out, heads_send, 1, EARLY)
    for weight in weights:
        weight.wait_send()
    for ref, lane in ((all_scalars, 0), (all_pieces, 1), (carried, 2)):
        landed(ref, send_sem.at[lane])


def body(*arrays):
    (
        stream,
        queries,
        key_rows,
        value_rows,
        out_gate,
        in_gate,
        forget_gate,
        out_proj,
        ffn_gain,
        gate_proj,
        up_proj,
        down_proj,
        expert_ids,
        route_weights,
    ) = arrays
    rows_here, width = stream.shape
    length = queries.shape[0]
    half = gate_proj.shape[2]
    slots = len(OFFSETS) * SLOT
    gain = ffn_gain.reshape(1, width)
    ids, routes = expert_ids.T, route_weights.T
    loaded = [
        stream,
        queries,
        key_rows,
        value_rows,
        out_gate,
        in_gate,
        forget_gate,
        out_proj,
        gain,
        ids,
        routes,
    ]
    vmem, dma = pltpu.VMEM, pltpu.SemaphoreType.DMA
    return pl.pallas_call(
        layer_kernel,
        out_shape=pltpu.VMEM((rows_here, width), BF16),
        in_specs=[pl.BlockSpec(memory_space=pl.ANY)] * 14,
        out_specs=pl.BlockSpec(memory_space=pltpu.VMEM),
        scratch_shapes=[vmem(a.shape, a.dtype) for a in loaded]
        + [
            vmem((128, length), F32),
            vmem((length, 128), F32),
            vmem((length, 2 * V_DIM), F32),
            vmem((2, length, 128), F32),
            vmem((length, 2 * V_DIM), F32),
            vmem((4, 128), F32),
            vmem((64, 4, 128), F32),
        ]
        + [vmem((64, 8, 128), F32)] * 4
        + [
            vmem((rows_here, 2 * V_DIM), BF16),
            vmem((rows_here, 4 * V_DIM), BF16),
            vmem((len(OFFSETS), rows_here), F32),
            vmem((len(OFFSETS), rows_here), F32),
            vmem((slots, rows_here), BF16),
            vmem((2, rows_here, slots), BF16),
            vmem((rows_here, width), BF16),
            vmem((rows_here, width), BF16),
        ]
        + [vmem((EARLY * SLOT, 4 * V_DIM), BF16)] * 2
        + [vmem((slots, width), BF16)] * 4
        + [
            vmem((width, 2 * half), BF16),
            vmem((width, 2 * half), BF16),
            vmem((2 * half, width), BF16),
            vmem((GROUP_ROWS, 2 * half), BF16),
            vmem((rows_here, width), F32),
            dma((14,)),
            dma((4,)),
            dma((4,)),
            dma((3,)),
            dma((3,)),
            dma(()),
            dma((GROUPS,)),
            dma((EARLY_GROUPS,)),
            dma(()),
            dma(()),
            dma((GROUPS,)),
        ],
        compiler_params=pltpu.CompilerParams(
            collective_id=0, has_side_effects=True, vmem_limit_bytes=62 << 20
        ),
    )(
        stream,
        queries,
        key_rows,
        value_rows,
        out_gate,
        in_gate,
        forget_gate,
        out_proj,
        gain,
        gate_proj[0],
        up_proj[0],
        down_proj[0],
        ids,
        routes,
    )


def solution(mesh):
    split = Mesh(mesh.devices.reshape(4, 4, 4, mesh.shape["tp"]), ("sp_0", "sp_1", "sp_2", "tp"))
    return jax.shard_map(
        body,
        mesh=split,
        in_specs=(
            P(SP_TP, None),
            P(SP, "tp"),
            P(SP, "tp"),
            P(SP, "tp"),
            P(SP, "tp"),
            P("tp", SP),
            P("tp", SP),
            P(),
            P(),
            P(SP, None, "tp"),
            P(SP, None, "tp"),
            P(SP, "tp", None),
            P(SP_TP, None),
            P(SP_TP, None),
        ),
        out_specs=P(SP_TP, None),
        check_vma=False,
    )
```

```python
import jax
import jax.numpy as jnp
from jax import lax
from jax.experimental import pallas as pl
from jax.experimental.pallas import tpu as pltpu
from jax.sharding import Mesh
from jax.sharding import PartitionSpec as P

MESH = pl.DeviceIdType.MESH
QK = 128
V_DIM = 256
SP = ("sp_0", "sp_1", "sp_2")
SP_TP = ("sp_0", "sp_1", "sp_2", "tp")
SLOT = 16
GROUP_ROWS = 256
PER_GROUP = GROUP_ROWS // SLOT
TILE = 256
epsilon = 1e-06
F32 = jnp.float32
BF16 = jnp.bfloat16


def offsets_by_orbit():
    cube = [(a, b, c) for a in range(4) for b in range(4) for c in range(4)]
    seen, orbits = {(0, 0, 0)}, []
    for o in sorted(cube, key=lambda o: sum(min(v, 4 - v) for v in o)):
        orbit = []
        for turn in range(3):
            turned = o[turn:] + o[:turn]
            for p in (turned, tuple(-v % 4 for v in turned)):
                if p not in seen:
                    seen.add(p)
                    orbit.append(p)
        if orbit:
            orbits.append(orbit)
    order = [(0, 0, 0)]
    for orbit in orbits:
        order += orbit
    return order


OFFSETS = offsets_by_orbit()
GROUPS = len(OFFSETS) // PER_GROUP
EARLY_GROUPS = 2
EARLY = EARLY_GROUPS * PER_GROUP
FIRST_WINDOW = 7


def place():
    return [lax.axis_index(axis) for axis in SP_TP]


def peer(here, offset, sign=1):
    z, y, x, core = here
    return tuple(lax.rem(p + (sign * o) % 4, 4) for p, o in zip((z, y, x), offset)) + (core,)


def index_of(device):
    return (device[0] * 4 + device[1]) * 4 + device[2]


FAR_FIRST = sorted(OFFSETS[1:], key=lambda o: -sum(min(v, 4 - v) for v in o))


def others(here, act):
    for offset in FAR_FIRST:
        device = peer(here, offset)
        act(index_of(device), device)


def route(ids_ref, routes_ref, ranks, shares, select_ref, weigh_ref, here, loads):
    loads["ids"].wait()
    loads["routes"].wait()
    named = ids_ref[...].astype(F32)
    tokens = named.shape[1]
    expert = lax.broadcasted_iota(jnp.int32, (len(OFFSETS), tokens), 0).astype(F32)
    first, second = (named[j : j + 1, :] == expert for j in range(2))
    used = jnp.where(first | second, 1.0, 0.0)
    earlier = lax.broadcasted_iota(jnp.int32, (tokens, tokens), 0)
    later = lax.broadcasted_iota(jnp.int32, (tokens, tokens), 1)
    upper = jnp.where(earlier < later, 1.0, 0.0).astype(BF16)
    rank = jnp.dot(used.astype(BF16), upper, preferred_element_type=F32)
    ranks[...] = jnp.where(first | second, rank, -1.0)
    shares[...] = jnp.where(first, routes_ref[0:1, :], 0.0) + jnp.where(second, routes_ref[1:2, :], 0.0)
    slot = lax.broadcasted_iota(jnp.int32, (SLOT, tokens), 0).astype(F32)
    for g in range(GROUPS):
        weights = []
        for i in range(g * PER_GROUP, (g + 1) * PER_GROUP):
            owner = pl.ds(index_of(peer(here, OFFSETS[i])), 1)
            chosen = ranks[owner, :] == slot
            select_ref[pl.ds(i * SLOT, SLOT), :] = jnp.where(chosen, 1.0, 0.0).astype(BF16)
            weights.append(jnp.where(chosen, shares[owner, :], 0.0))
        weigh = jnp.concatenate(weights, axis=0).T
        high = weigh.astype(BF16)
        cols = slice(g * GROUP_ROWS, (g + 1) * GROUP_ROWS)
        weigh_ref[0, :, cols] = high
        weigh_ref[1, :, cols] = (weigh - high.astype(F32)).astype(BF16)


def layer_kernel(
    stream_hbm,
    query_hbm,
    key_hbm,
    value_hbm,
    out_gate_hbm,
    in_gate_hbm,
    forget_hbm,
    out_proj_hbm,
    gain_hbm,
    gate_ref,
    up_ref,
    down_ref,
    ids_hbm,
    routes_hbm,
    out_ref,
    stream_ref,
    query_ref,
    key_ref,
    value_ref,
    out_gate_ref,
    in_gate_ref,
    forget_ref,
    out_proj_ref,
    gain_ref,
    ids_ref,
    routes_ref,
    table,
    columns,
    local_num,
    local_level,
    gates_ref,
    scalars,
    all_scalars,
    pieces,
    all_pieces,
    carries,
    carried,
    outbox,
    heads,
    ranks,
    shares,
    select_ref,
    weigh_ref,
    middle_ref,
    normed_ref,
    slots_out,
    slots_in,
    outgoing,
    arrived,
    answers,
    returned,
    gate_full,
    up_full,
    down_full,
    hidden,
    total,
    load_sem,
    send_sem,
    recv_sem,
    weight_send,
    weight_recv,
    rows_send,
    rows_recv,
    early_recv,
    heads_send,
    back_send,
    back_recv,
):
    here = place()
    core = here[3]
    me = index_of(here)
    partner = (here[0], here[1], here[2], 1 - core)
    units = gate_ref.shape[1]
    barrier = pltpu.get_barrier_semaphore()
    others(
        here,
        lambda d, dev: pl.semaphore_signal(barrier, inc=1, device_id=dev, device_id_type=MESH),
    )
    pl.semaphore_signal(barrier, inc=1, device_id=partner, device_id_type=MESH)
    loads = {}
    for name, src, dst in (
        ("forget", forget_hbm, forget_ref),
        ("in", in_gate_hbm, in_gate_ref),
        ("key", key_hbm, key_ref),
        ("value", value_hbm, value_ref),
        ("ids", ids_hbm, ids_ref),
        ("routes", routes_hbm, routes_ref),
        ("stream", stream_hbm, stream_ref),
        ("query", query_hbm, query_ref),
        ("out_gate", out_gate_hbm, out_gate_ref),
        ("out_proj", out_proj_hbm, out_proj_ref),
        ("gain", gain_hbm, gain_ref),
        ("gate", gate_ref, gate_full.at[:, pl.ds(0, units)]),
        ("up", up_ref, up_full.at[:, pl.ds(0, units)]),
        ("down", down_ref, down_full.at[pl.ds(0, units)]),
    ):
        loads[name] = pltpu.make_async_copy(src, dst, load_sem.at[len(loads)])
        loads[name].start()

    length = query_ref.shape[0]
    scale = QK ** (-0.5)
    loads["forget"].wait()
    loads["in"].wait()
    x = forget_ref[...]
    u = jnp.exp(-jnp.abs(x))
    small = u * (1.0 - u * (0.5 - u * (1.0 / 3.0 - u * 0.25)))
    decay = jnp.minimum(x, 0.0) - jnp.where(u < 0.01, small, jnp.log(1.0 + u))
    table[...] = jnp.zeros_like(table)
    table[0:2, :] = decay
    raw = table[0:8, :]
    high = raw.astype(jnp.bfloat16).astype(jnp.float32)
    mid = (raw - high).astype(jnp.bfloat16).astype(jnp.float32)
    low = raw - high - mid
    parts = jnp.concatenate([high, mid, low], axis=0).astype(jnp.bfloat16)
    before = lax.broadcasted_iota(jnp.int32, (length, length), 0)
    after = lax.broadcasted_iota(jnp.int32, (length, length), 1)
    upper = jnp.where(before <= after, 1.0, 0.0).astype(jnp.bfloat16)
    summed = jnp.dot(parts, upper, preferred_element_type=jnp.float32)
    summed = summed[0:8] + summed[8:16] + summed[16:24]
    table[0:2, :] = summed[0:2]
    table[2:4, :] = in_gate_ref[...]
    columns[...] = table[...].T
    rows_a, peaks = [], []
    for h in range(2):
        row_a = table[2 + h : 3 + h, :] - table[h : h + 1, :]
        peak = jnp.max(row_a, axis=1, keepdims=True)
        closing = table[h : h + 1, length - 1 : length]
        scalars[h : h + 1, :] = jnp.broadcast_to(closing + peak, (1, 128))
        scalars[2 + h : 3 + h, :] = jnp.broadcast_to(closing, (1, 128))
        rows_a.append(row_a)
        peaks.append(peak)
    loads["key"].wait()
    loads["value"].wait()
    for h in range(2):
        col_a = columns[:, 2 + h : 3 + h] - columns[:, h : h + 1]
        weight = jnp.exp(col_a - peaks[h]) * scale
        keys = (key_ref[:, h * QK : (h + 1) * QK].astype(jnp.float32) * weight).astype(jnp.bfloat16)
        state = lax.dot_general(
            keys,
            value_ref[:, h * V_DIM : (h + 1) * V_DIM],
            (((0,), (0,)), ((), ())),
            preferred_element_type=jnp.float32,
        )
        for half in range(2):
            at = h * 32 + half * 16
            pieces[at : at + 16] = state[:, half * 128 : (half + 1) * 128].reshape(16, 8, 128)
    route(ids_ref, routes_ref, ranks, shares, select_ref, weigh_ref, here, loads)
    width = stream_ref.shape[1]
    tiles = [slice(n, n + TILE) for n in range(0, width, TILE)]

    def spot(i):
        return pl.ds(i * SLOT, SLOT)

    def group(g):
        return pl.ds(g * GROUP_ROWS, GROUP_ROWS)

    def members(g):
        return range(max(g * PER_GROUP, 1), (g + 1) * PER_GROUP)

    def fill(g, source, target):
        pick = select_ref[group(g), :]
        for n in range(0, source.shape[1], TILE):
            cols = slice(n, n + TILE)
            target[group(g), cols] = jnp.dot(
                pick, source[:, cols], preferred_element_type=F32
            ).astype(BF16)

    def push(source, target, blocks, sends, lands, sign=1):
        for i in blocks:
            pltpu.make_async_remote_copy(
                src_ref=source.at[spot(i)],
                dst_ref=target.at[spot(i)],
                send_sem=sends,
                recv_sem=lands,
                device_id=peer(here, OFFSETS[i], sign),
                device_id_type=MESH,
            ).start()

    def all_in(ref, sem, first, last):
        span = ref.at[pl.ds(first * SLOT, (last - first) * SLOT)]
        pltpu.make_async_copy(span, span, sem).wait()

    loads["stream"].wait()
    for g in range(EARLY_GROUPS):
        fill(g, stream_ref, outgoing)
    arrived[spot(0), :] = outgoing[spot(0), :]
    pl.semaphore_wait(barrier, 64)

    def copy(src, dst, lane, dev):
        return pltpu.make_async_remote_copy(
            src_ref=src,
            dst_ref=dst,
            send_sem=send_sem.at[lane],
            recv_sem=recv_sem.at[lane],
            device_id=dev,
            device_id_type=MESH,
        )

    def landed(ref, sem):
        span = ref.at[pl.ds(0, 63)]
        pltpu.make_async_copy(span, span, sem).wait()

    def spread(d, dev):
        copy(scalars, all_scalars.at[me], 0, dev).start()
        copy(pieces.at[d], all_pieces.at[me], 1, dev).start()

    others(here, spread)
    for g in range(EARLY_GROUPS):
        push(outgoing, arrived, [i for i in members(g) if i < FIRST_WINDOW], rows_send, early_recv.at[g])
    all_scalars[me] = scalars[...]
    all_pieces[me] = pieces[me]

    loads["query"].wait()
    step = 128
    for h in range(2):
        for r in range(length // step):
            n = (r + 1) * step
            rows = slice(r * step, n)
            score = lax.dot_general(
                query_ref[rows, h * QK : (h + 1) * QK],
                key_ref[0:n, h * QK : (h + 1) * QK],
                (((1,), (1,)), ((), ())),
                preferred_element_type=jnp.float32,
            )
            t = lax.broadcasted_iota(jnp.int32, (step, n), 0) + r * step
            s = lax.broadcasted_iota(jnp.int32, (step, n), 1)
            log_inner = jnp.where(s <= t, columns[rows, h : h + 1] + rows_a[h][:, 0:n], -1e30)
            level = jnp.max(log_inner, axis=1, keepdims=True)
            score = (score * scale * jnp.exp(log_inner - level)).astype(jnp.bfloat16)
            local_num[rows, h * V_DIM : (h + 1) * V_DIM] = jnp.dot(
                score, value_ref[0:n, h * V_DIM : (h + 1) * V_DIM], preferred_element_type=jnp.float32
            )
            local_level[h, rows, :] = jnp.broadcast_to(level, (step, 128))

    landed(all_scalars, recv_sem.at[0])

    def climb(s, level):
        new = jnp.maximum(all_scalars[s, 2:4, :] + level, all_scalars[s, 0:2, :])
        return jnp.where(s < me, new, level)

    landed(all_pieces, recv_sem.at[1])
    head = me // 32

    def scan(s, held):
        state, level = held
        carries[s] = state
        late = all_scalars[s, pl.ds(head, 1), :]
        moved = all_scalars[s, pl.ds(2 + head, 1), :] + level
        new = jnp.maximum(moved, late)
        state = state * jnp.exp(moved - new) + all_pieces[s] * jnp.exp(late - new)
        return (state, new)

    nothing = (jnp.zeros((8, 128), jnp.float32), jnp.zeros((1, 128), jnp.float32))
    lax.fori_loop(0, 64, scan, nothing, unroll=4)
    others(here, lambda d, dev: copy(carries.at[d], carried.at[me], 2, dev).start())
    weights = [
        pltpu.make_async_remote_copy(
            src_ref=mine_,
            dst_ref=theirs,
            send_sem=weight_send.at[i],
            recv_sem=weight_recv.at[i],
            device_id=partner,
            device_id_type=MESH,
        )
        for i, (mine_, theirs) in enumerate(
            (
                (gate_ref, gate_full.at[:, pl.ds(units, units)]),
                (up_ref, up_full.at[:, pl.ds(units, units)]),
                (down_ref, down_full.at[pl.ds(units, units)]),
            )
        )
    ]
    for weight in weights:
        weight.start()
    for g in range(EARLY_GROUPS):
        push(outgoing, arrived, [i for i in members(g) if i >= FIRST_WINDOW], rows_send, early_recv.at[g])
    carried[me] = carries[me]
    anchor = lax.fori_loop(0, 64, climb, jnp.zeros((2, 128), jnp.float32), unroll=4)
    loads["out_gate"].wait()
    for h in range(2):
        wide = slice(h * V_DIM, (h + 1) * V_DIM)
        log_inter = columns[:, h : h + 1] + anchor[h : h + 1, 0:1]
        level = local_level[h, :, 0:1]
        peak = jnp.maximum(log_inter, level)
        local_num[:, wide] = jnp.exp(level - peak) * local_num[:, wide]
        local_level[h] = jnp.broadcast_to(jnp.exp(log_inter - peak), (length, 128))
        gates_ref[:, wide] = jax.nn.sigmoid(out_gate_ref[:, wide].astype(F32))
    landed(carried, recv_sem.at[2])

    span = length // 2

    def finish(start, store):
        rows = pl.ds(pl.multiple_of(start, span), span)
        for h in range(2):
            state = jnp.concatenate(
                [
                    carried[h * 32 + half * 16 : h * 32 + (half + 1) * 16].reshape(QK, 128)
                    for half in range(2)
                ],
                axis=1,
            ).astype(jnp.bfloat16)
            wide = slice(h * V_DIM, (h + 1) * V_DIM)
            from_state = jnp.dot(
                query_ref[rows, h * QK : (h + 1) * QK], state, preferred_element_type=jnp.float32
            )
            number = local_level[h, rows, 0:1] * from_state + local_num[rows, wide]
            scaled = number * lax.rsqrt(
                jnp.mean(number * number, axis=1, keepdims=True) + epsilon
            )
            store(h, (scaled * gates_ref[rows, wide]).astype(jnp.bfloat16))

    def to_partner(h, value):
        outbox[:, h * V_DIM : (h + 1) * V_DIM] = value

    def to_self(h, value):
        start = pl.multiple_of(core * 2 * V_DIM + h * V_DIM, V_DIM)
        heads[:, pl.ds(start, V_DIM)] = value

    finish((1 - core) * span, to_partner)
    mine = pl.ds(pl.multiple_of(core * 2 * V_DIM, 2 * V_DIM), 2 * V_DIM)
    swap = copy(outbox, heads.at[:, mine], 3, partner)
    swap.start()
    finish(core * span, to_self)
    swap.wait()
    for g in range(EARLY_GROUPS):
        fill(g, heads, slots_out)
        push(slots_out, slots_in, members(g), heads_send, rows_recv.at[g])
    slots_in[spot(0), :] = slots_out[spot(0), :]
    loads["out_proj"].wait()
    loads["gain"].wait()
    squares = jnp.zeros((stream_ref.shape[0], 1), F32)
    for cols in tiles:
        mix = jnp.dot(heads[...], out_proj_ref[:, cols], preferred_element_type=F32)
        both = (stream_ref[:, cols].astype(F32) + mix).astype(BF16)
        middle_ref[:, cols] = both
        both = both.astype(F32)
        squares = squares + jnp.sum(both * both, axis=1, keepdims=True)
    factor = lax.rsqrt(squares / width + epsilon)
    for cols in tiles:
        normed_ref[:, cols] = (middle_ref[:, cols].astype(F32) * factor * gain_ref[:, cols]).astype(BF16)

    for g in range(EARLY_GROUPS, GROUPS):
        fill(g, normed_ref, outgoing)
        push(outgoing, arrived, members(g), rows_send, rows_recv.at[g])

    for name in ("gate", "up", "down"):
        loads[name].wait()
    for weight in weights:
        weight.wait_recv()
    for g in range(GROUPS):
        if g < EARLY_GROUPS:
            first = members(g)[0]
            all_in(arrived, early_recv.at[g], first, (g + 1) * PER_GROUP)
            all_in(slots_in, rows_recv.at[g], first, (g + 1) * PER_GROUP)
            squares = jnp.zeros((GROUP_ROWS, 1), F32)
            for cols in tiles:
                mix = jnp.dot(slots_in[group(g), :], out_proj_ref[:, cols], preferred_element_type=F32)
                both = (arrived[group(g), cols].astype(F32) + mix).astype(BF16)
                arrived[group(g), cols] = both
                both = both.astype(F32)
                squares = squares + jnp.sum(both * both, axis=1, keepdims=True)
            factor = lax.rsqrt(squares / width + epsilon)
            for cols in tiles:
                arrived[group(g), cols] = (
                    arrived[group(g), cols].astype(F32) * factor * gain_ref[:, cols]
                ).astype(BF16)
        else:
            all_in(arrived, rows_recv.at[g], members(g)[0], members(g)[-1] + 1)
        block = arrived[group(g), :]
        for n in range(0, hidden.shape[1], TILE):
            cols = slice(n, n + TILE)
            gates = jnp.dot(block, gate_full[:, cols], preferred_element_type=F32)
            ups = jnp.dot(block, up_full[:, cols], preferred_element_type=F32)
            hidden[:, cols] = (gates * jax.nn.sigmoid(gates) * ups).astype(BF16)
        for cols in tiles:
            answers[group(g), cols] = jnp.dot(
                hidden[...], down_full[:, cols], preferred_element_type=F32
            ).astype(BF16)
        push(answers, returned, members(g), back_send, back_recv.at[g], -1)
    returned[spot(0), :] = answers[spot(0), :]
    for g in range(GROUPS):
        all_in(returned, back_recv.at[g], members(g)[0], members(g)[-1] + 1)
        for cols in tiles:
            part = jnp.dot(
                weigh_ref[0, :, group(g)], returned[group(g), cols], preferred_element_type=F32
            ) + jnp.dot(
                weigh_ref[1, :, group(g)], returned[group(g), cols], preferred_element_type=F32
            )
            before = middle_ref[:, cols].astype(F32) if g == 0 else total[:, cols]
            if g < GROUPS - 1:
                total[:, cols] = before + part
            else:
                out_ref[:, cols] = (before + part).astype(out_ref.dtype)
    all_in(outgoing, rows_send, 1, len(OFFSETS))
    all_in(answers, back_send, 1, len(OFFSETS))
    all_in(slots_out, heads_send, 1, EARLY)
    for weight in weights:
        weight.wait_send()
    for ref, lane in ((all_scalars, 0), (all_pieces, 1), (carried, 2)):
        landed(ref, send_sem.at[lane])


def body(*arrays):
    (
        stream,
        queries,
        key_rows,
        value_rows,
        out_gate,
        in_gate,
        forget_gate,
        out_proj,
        ffn_gain,
        gate_proj,
        up_proj,
        down_proj,
        expert_ids,
        route_weights,
    ) = arrays
    rows_here, width = stream.shape
    length = queries.shape[0]
    half = gate_proj.shape[2]
    slots = len(OFFSETS) * SLOT
    gain = ffn_gain.reshape(1, width)
    ids, routes = expert_ids.T, route_weights.T
    loaded = [
        stream,
        queries,
        key_rows,
        value_rows,
        out_gate,
        in_gate,
        forget_gate,
        out_proj,
        gain,
        ids,
        routes,
    ]
    vmem, dma = pltpu.VMEM, pltpu.SemaphoreType.DMA
    return pl.pallas_call(
        layer_kernel,
        out_shape=pltpu.VMEM((rows_here, width), BF16),
        in_specs=[pl.BlockSpec(memory_space=pl.ANY)] * 14,
        out_specs=pl.BlockSpec(memory_space=pltpu.VMEM),
        scratch_shapes=[vmem(a.shape, a.dtype) for a in loaded]
        + [
            vmem((128, length), F32),
            vmem((length, 128), F32),
            vmem((length, 2 * V_DIM), F32),
            vmem((2, length, 128), F32),
            vmem((length, 2 * V_DIM), F32),
            vmem((4, 128), F32),
            vmem((64, 4, 128), F32),
        ]
        + [vmem((64, 8, 128), F32)] * 4
        + [
            vmem((rows_here, 2 * V_DIM), BF16),
            vmem((rows_here, 4 * V_DIM), BF16),
            vmem((len(OFFSETS), rows_here), F32),
            vmem((len(OFFSETS), rows_here), F32),
            vmem((slots, rows_here), BF16),
            vmem((2, rows_here, slots), BF16),
            vmem((rows_here, width), BF16),
            vmem((rows_here, width), BF16),
        ]
        + [vmem((EARLY * SLOT, 4 * V_DIM), BF16)] * 2
        + [vmem((slots, width), BF16)] * 4
        + [
            vmem((width, 2 * half), BF16),
            vmem((width, 2 * half), BF16),
            vmem((2 * half, width), BF16),
            vmem((GROUP_ROWS, 2 * half), BF16),
            vmem((rows_here, width), F32),
            dma((14,)),
            dma((4,)),
            dma((4,)),
            dma((3,)),
            dma((3,)),
            dma(()),
            dma((GROUPS,)),
            dma((EARLY_GROUPS,)),
            dma(()),
            dma(()),
            dma((GROUPS,)),
        ],
        compiler_params=pltpu.CompilerParams(
            collective_id=0, has_side_effects=True, vmem_limit_bytes=62 << 20
        ),
    )(
        stream,
        queries,
        key_rows,
        value_rows,
        out_gate,
        in_gate,
        forget_gate,
        out_proj,
        gain,
        gate_proj[0],
        up_proj[0],
        down_proj[0],
        ids,
        routes,
    )


def solution(mesh):
    split = Mesh(mesh.devices.reshape(4, 4, 4, mesh.shape["tp"]), ("sp_0", "sp_1", "sp_2", "tp"))
    return jax.shard_map(
        body,
        mesh=split,
        in_specs=(
            P(SP_TP, None),
            P(SP, "tp"),
            P(SP, "tp"),
            P(SP, "tp"),
            P(SP, "tp"),
            P("tp", SP),
            P("tp", SP),
            P(),
            P(),
            P(SP, None, "tp"),
            P(SP, None, "tp"),
            P(SP, "tp", None),
            P(SP_TP, None),
            P(SP_TP, None),
        ),
        out_specs=P(SP_TP, None),
        check_vma=False,
    )
```
